512 devices in a mesh: rep: 2 (over z_hi), fs: 32 (over z_lo, y), tp: 8 (over x, core).
Axes of the slice: x: 4, y: 8, z: 8 (z_hi: 2, z_lo: 4; z = z_hi * 4 + z_lo), core: 2. Of those that a mesh axis runs over, the one named last changes fastest.
Arguments:
- tokens: bfloat16 [64, 384, 2048], P(('rep', 'fs')), may hold values from -6 to 6
- mix_gain: float32 [2048], replicated, may hold values from 0.1 to 1.9
- value_weight: float32 [2048, 2048], P('fs', 'tp'), may hold values from -0.125 to 0.125
- value_scale: float32 [2048], P(('tp', 'fs')), may hold values from 0.5 to 2
- inner_weight: float32 [2048, 2048], P('fs', 'tp'), may hold values from -0.125 to 0.125
- inner_scale: float32 [2048], P(('tp', 'fs')), may hold values from 0.5 to 2
- outer_weight: float32 [2048, 2048], P('fs', 'tp'), may hold values from -0.125 to 0.125
- outer_scale: float32 [2048], P(('tp', 'fs')), may hold values from 0.5 to 2
- conv_taps: float32 [3, 2048], P(None, 'tp'), may hold values from -3 to 3
- out_weight: float32 [2048, 2048], P('tp', 'fs'), may hold values from -0.125 to 0.125
- out_scale: float32 [2048], P('fs'), may hold values from 0.5 to 2
- mlp_gain: float32 [2048], replicated, may hold values from 0.1 to 1.9
- up_weight: float32 [2048, 6144], P('fs', 'tp'), may hold values from -0.125 to 0.125
- up_scale: float32 [6144], P(('tp', 'fs')), may hold values from 0.5 to 2
- down_weight: float32 [6144, 2048], P('tp', 'fs'), may hold values from -0.078125 to 0.078125
- down_scale: float32 [2048], P('fs'), may hold values from 0.5 to 2
Outputs:
- layer_out: bfloat16 [64, 384, 2048], P(('rep', 'fs'))
The draws below stay inside these ranges and needn't reach their ends.
All inputs are finite; a program needn't handle non-finite values.
Results may differ from the reference program's by a relative error of at most 0.02.
Values may be sent and summed in bfloat16 or wider, within the bound.
No kernel may reach another device: no remote copies, remote signals or barrier semaphores. Data moves between devices by JAX's collectives and lax.ppermute only.
A program may use at most 64 MiB of HBM per device.

```python
import math
import jax
import jax.numpy as jnp
from jax import lax

D = 2048
FF = 6144
TOK_DEV = 384
SEQS = 64
N_TP = 8


def block_scale(rng, dims, shards, low, high):
    def one(axis_at, shards_of):
        heights = jax.random.uniform(jax.random.fold_in(jax.random.fold_in(rng, 6), axis_at), (shards_of,), jnp.float32, low / len(shards), high / len(shards))
        return jnp.repeat(jnp.exp(heights), dims[axis_at] // shards_of).reshape((-1,) + (1,) * (len(dims) - axis_at - 1))

    level = one(*shards[0])
    for cut in shards[1:]:
        level = level * one(*cut)
    return level


def scatter_about(key, shape, scale, limit, cuts=(), kind=jnp.bfloat16):
    values = scale * jax.random.normal(key, shape, jnp.float32)
    if cuts:
        values = values * block_scale(key, shape, cuts, -0.22, 0.18)
    return jnp.clip(values, -limit, limit).astype(kind)


def setup_inputs(seed: int = 0) -> dict:
    key_of = jax.random.split(jax.random.key(seed), 17)
    return {
        "tokens": scatter_about(key_of[0], (SEQS, TOK_DEV, D), 1.0, 6.0, ((0, 64),)),
        "mix_gain": jnp.clip(1.0 + 0.18 * jax.random.normal(key_of[1], (D,), jnp.float32), 0.1, 1.9),
        "value_weight": scatter_about(key_of[2], (D, D), D ** -0.5, 0.125, ((0, 32), (1, 8)), jnp.float32),
        "value_scale": jnp.clip(jnp.exp(math.log(2.0) - 1.3862944 * jax.random.uniform(key_of[3], (D,), jnp.float32) ** block_scale(key_of[3], (D,), ((0, 256),), -0.2, 0.2)), 0.5, 2.0),
        "inner_weight": scatter_about(key_of[4], (D, D), D ** -0.5, 0.125, ((0, 32), (1, 8)), jnp.float32),
        "inner_scale": jnp.clip(jnp.exp(math.log(2.0) - 1.3862944 * jax.random.uniform(key_of[5], (D,), jnp.float32) ** block_scale(key_of[5], (D,), ((0, 256),), -0.2, 0.2)), 0.5, 2.0),
        "outer_weight": scatter_about(key_of[6], (D, D), D ** -0.5, 0.125, ((0, 32), (1, 8)), jnp.float32),
        "outer_scale": jnp.clip(jnp.exp(math.log(2.0) - 1.3862944 * jax.random.uniform(key_of[7], (D,), jnp.float32) ** block_scale(key_of[7], (D,), ((0, 256),), -0.2, 0.2)), 0.5, 2.0),
        "conv_taps": scatter_about(key_of[8], (3, D), 0.6, 3.0, ((1, 8),), jnp.float32),
        "out_weight": scatter_about(key_of[9], (D, D), D ** -0.5, 0.125, ((0, 8), (1, 32)), jnp.float32),
        "out_scale": jnp.clip(jnp.exp(math.log(2.0) - 1.3862944 * jax.random.uniform(key_of[10], (D,), jnp.float32) ** block_scale(key_of[10], (D,), ((0, 32),), -0.2, 0.2)), 0.5, 2.0),
        "mlp_gain": jnp.clip(1.0 + 0.18 * jax.random.normal(key_of[11], (D,), jnp.float32), 0.1, 1.9),
        "up_weight": scatter_about(key_of[12], (D, FF), D ** -0.5, 0.125, ((0, 32), (1, 8)), jnp.float32),
        "up_scale": jnp.clip(jnp.exp(math.log(2.0) - 1.3862944 * jax.random.uniform(key_of[13], (FF,), jnp.float32) ** block_scale(key_of[13], (FF,), ((0, 256),), -0.2, 0.2)), 0.5, 2.0),
        "down_weight": scatter_about(key_of[14], (FF, D), FF ** -0.5, 0.078125, ((0, 8), (1, 32)), jnp.float32),
        "down_scale": jnp.clip(jnp.exp(math.log(2.0) - 1.3862944 * jax.random.uniform(key_of[15], (D,), jnp.float32) ** block_scale(key_of[15], (D,), ((0, 32),), -0.2, 0.2)), 0.5, 2.0),
    }


norm_eps = 1e-06

def normalize(values, gain):
    return values * lax.rsqrt(lax.optimization_barrier(jnp.mean(values * values, axis=-1, keepdims=True)) + norm_eps) * gain

def block_sum(left, right, blocks):
    rows = left.shape[0]
    width = left.shape[1] // blocks
    left_blocks = left.reshape(rows, blocks, width).astype(jnp.float32)
    right_blocks = right.reshape(blocks, width, right.shape[1]).astype(jnp.float32)
    parts = jnp.einsum('lnk,nkd->nld', left_blocks, right_blocks).astype(jnp.bfloat16)
    parts = lax.optimization_barrier(parts)
    return lax.optimization_barrier(jnp.sum(parts.astype(jnp.float32), axis=0))

def reference(tokens, mix_gain, value_weight, value_scale, inner_weight, inner_scale, outer_weight, outer_scale, conv_taps, out_weight, out_scale, mlp_gain, up_weight, up_scale, down_weight, down_scale):
    value_b = value_weight.astype(jnp.bfloat16)
    inner_b = inner_weight.astype(jnp.bfloat16)
    outer_b = outer_weight.astype(jnp.bfloat16)
    out_b = out_weight.astype(jnp.bfloat16)
    up_b = up_weight.astype(jnp.bfloat16)
    down_b = down_weight.astype(jnp.bfloat16)

    def one_sequence(sequence):
        start = sequence.astype(jnp.float32)
        normed = normalize(start, mix_gain).astype(jnp.bfloat16)
        value = jnp.dot(normed, value_b, preferred_element_type=jnp.float32) * value_scale
        inner = jnp.dot(normed, inner_b, preferred_element_type=jnp.float32) * inner_scale
        outer = jnp.dot(normed, outer_b, preferred_element_type=jnp.float32) * outer_scale
        gated = inner * value
        padded = jnp.pad(gated, ((1, 1), (0, 0)))
        conv = conv_taps[0] * padded[:-2] + conv_taps[1] * padded[1:-1] + conv_taps[2] * padded[2:]
        hidden = (outer * conv).astype(jnp.bfloat16)
        middle = start + block_sum(hidden, out_b, N_TP) * out_scale
        normed_mid = normalize(middle, mlp_gain).astype(jnp.bfloat16)
        upper = jnp.dot(normed_mid, up_b, preferred_element_type=jnp.float32) * up_scale
        act = jnp.square(jax.nn.relu(upper)).astype(jnp.bfloat16)
        return (middle + block_sum(act, down_b, N_TP) * down_scale).astype(jnp.bfloat16)
    return lax.map(one_sequence, tokens)
```

```python
import jax
import jax.numpy as jnp
from jax import lax
from jax.sharding import Mesh, PartitionSpec as P

norm_eps = 1e-06

Z = ("zh", "zl")
FS = ("zl", "y")
BF = jnp.bfloat16
F32 = jnp.float32


def z_shift(a, step):
    return lax.ppermute(a, Z, [(i, (i + step) % 8) for i in range(8)])


def swap_cores(a):
    return lax.ppermute(a, "c", [(0, 1), (1, 0)])


def everyone(a, axis):
    copies = jnp.broadcast_to(a, (lax.axis_size(axis), *a.shape))
    return lax.all_to_all(copies, axis, 0, 0, tiled=True)


def along_z(a):
    half = a.shape[0] // 2
    before = z_shift(a, 1)
    after = z_shift(a, -1)
    far_low = z_shift(before[:half], 1)
    far_high = z_shift(after[half:], -1)
    return [a, after, far_low, far_high, before]


def gather_y_z(a):
    got = everyone(a, "y")
    return along_z(got.reshape(-1, a.shape[1]))


def rotated(v, z):
    blocks = [lax.dynamic_slice_in_dim(v, (z + k) % 4 * 512, 512, v.ndim - 1) for k in range(4)]
    return jnp.concatenate(blocks, axis=-1)


def normalize(values, gain):
    return values * lax.rsqrt(jnp.mean(values * values, axis=-1, keepdims=True) + norm_eps) * gain


def dot(a, b):
    return jnp.dot(a, b, preferred_element_type=F32)


def dot_t(a, b):
    return lax.dot_general(a, b, (((1,), (1,)), ((), ())), preferred_element_type=F32)


def times_rows(a, pieces):
    total, at = None, 0
    for p in pieces:
        part = dot(a[:, at : at + p.shape[0]], p)
        total = part if total is None else total + part
        at += p.shape[0]
    return total


def times_cols(a, pieces):
    return jnp.concatenate([dot_t(a, p) for p in pieces], axis=1)


def body(
    tokens,
    mix_gain,
    value_weight,
    value_scale,
    inner_weight,
    inner_scale,
    outer_weight,
    outer_scale,
    conv_taps,
    out_weight,
    out_scale,
    mlp_gain,
    up_weight,
    up_scale,
    down_weight,
    down_scale,
):
    z = lax.axis_index("zl")
    x = lax.axis_index("x")
    c = lax.axis_index("c")
    vi = jnp.concatenate([value_weight.astype(BF), inner_weight.astype(BF)], axis=1)
    ob = outer_weight.astype(BF)
    vi_pieces = gather_y_z(vi)
    ob_z = [ob, z_shift(ob, -1), z_shift(ob, 2), z_shift(ob, 1)]
    outer_all = everyone(jnp.stack(ob_z), "y")
    outer_all = jnp.moveaxis(outer_all.reshape(8, 4, 64, 256), 1, 0).reshape(2048, 256)
    scales = jnp.concatenate([value_scale, inner_scale, outer_scale, up_scale, out_scale, down_scale])
    scales = everyone(scales[None], FS).reshape(32, 176)
    out_pieces = gather_y_z(out_weight.T.astype(BF))
    up_pieces = gather_y_z(up_weight.astype(BF))
    down_pieces = gather_y_z(down_weight.T.astype(BF))

    value_cols = scales[:, 0:8].reshape(256)
    inner_cols = scales[:, 8:16].reshape(256)
    outer_cols = scales[:, 16:24].reshape(256)
    up_cols = scales[:, 24:48].reshape(768)
    out_cols = rotated(scales[:, 48:112].reshape(2048), z)
    down_cols = rotated(scales[:, 112:176].reshape(2048), z)

    tok = rotated(tokens[0], z)
    normed = normalize(tok.astype(F32), rotated(mix_gain, z)).astype(BF)
    share = lax.dynamic_slice_in_dim(tok, c * 192 + x * 48, 48, 0).astype(F32)

    both = times_rows(normed, vi_pieces)
    gated = both[:, 256:] * inner_cols * (both[:, :256] * value_cols)
    outer = dot(normed, outer_all)
    border = jnp.zeros((1, 256), F32)
    before = jnp.concatenate([border, gated[:-1]], axis=0)
    after = jnp.concatenate([gated[1:], border], axis=0)
    conv = conv_taps[0] * before + conv_taps[1] * gated + conv_taps[2] * after
    hidden = (outer * outer_cols * conv).astype(BF)

    hidden_own = lax.dynamic_slice_in_dim(hidden, c * 192, 192, 0)
    hidden_other = lax.dynamic_slice_in_dim(hidden, (1 - c) * 192, 192, 0)
    mix_other = swap_cores(times_cols(hidden_other, out_pieces).astype(BF))
    mix_own = times_cols(hidden_own, out_pieces)
    mix = (mix_own + mix_other.astype(F32)).astype(BF)
    mix = lax.all_to_all(mix.reshape(4, 48, 2048), "x", 0, 0, tiled=True)
    middle = share + mix.astype(F32).sum(axis=0) * out_cols
    normed_share = normalize(middle, rotated(mlp_gain, z)).astype(BF)

    own = everyone(normed_share, "x").reshape(192, 2048)
    other = swap_cores(own)

    def act_of(rows):
        return jnp.square(jax.nn.relu(times_rows(rows, up_pieces) * up_cols)).astype(BF)

    act_own = act_of(own)
    mlp_other = swap_cores(times_cols(act_of(other), down_pieces).astype(BF))
    mlp = (times_cols(act_own, down_pieces) + mlp_other.astype(F32)).astype(BF)
    mlp = lax.all_to_all(mlp.reshape(4, 48, 2048), "x", 0, 0, tiled=True)
    out_share = (middle + mlp.astype(F32).sum(axis=0) * down_cols).astype(BF)
    out_share = rotated(out_share, (4 - z) % 4)
    mine = everyone(out_share, "x").reshape(192, 2048)
    theirs = swap_cores(mine)
    result = jnp.zeros((384, 2048), BF)
    result = lax.dynamic_update_slice_in_dim(result, mine, c * 192, 0)
    result = lax.dynamic_update_slice_in_dim(result, theirs, (1 - c) * 192, 0)
    return result[None]


def solution(mesh):
    fine = Mesh(mesh.devices.reshape(2, 4, 8, 4, 2), ("zh", "zl", "y", "x", "c"))
    rows = P(("zh", "zl", "y"), None, None)
    fs, tp = ("zl", "y"), ("x", "c")
    all_cols = P(tp + fs)
    placed = (
        rows,
        P(),
        P(fs, tp),
        all_cols,
        P(fs, tp),
        all_cols,
        P(fs, tp),
        all_cols,
        P(None, tp),
        P(tp, fs),
        P(fs),
        P(),
        P(fs, tp),
        all_cols,
        P(tp, fs),
        P(fs),
    )
    return jax.shard_map(body, mesh=fine, in_specs=placed, out_specs=rows, check_vma=False)
```

```python
import jax
import jax.numpy as jnp
from jax import lax
from jax.experimental import pallas as pl
from jax.experimental.pallas import tpu as pltpu
from jax.sharding import Mesh, PartitionSpec as P


norm_eps = 1e-06

Z = ("zh", "zl")
FS = ("zl", "y")
BF = jnp.bfloat16
F32 = jnp.float32
SHAPE = jax.ShapeDtypeStruct


def z_shift(a, step):
    return lax.ppermute(a, Z, [(i, (i + step) % 8) for i in range(8)])


def swap_cores(a):
    return lax.ppermute(a, "c", [(0, 1), (1, 0)])


def spread(a, axis):
    return lax.all_to_all(a, axis, 0, 0, tiled=True)


def everyone(a, axis):
    return spread(jnp.broadcast_to(a, (lax.axis_size(axis), *a.shape)), axis)


def along_z(got):
    half = got.shape[0] // 2
    before = z_shift(got, 1)
    after = z_shift(got, -1)
    far_low = z_shift(before[:half], 1)
    far_high = z_shift(after[half:], -1)
    return [after, far_low, far_high, before]


def kernel(body, outs, flops, *args, weights=(), scratch=(), limit=24):
    spaces = [pltpu.SMEM if a.dtype == jnp.int32 else pltpu.VMEM for a in args]
    weights = [w if isinstance(w, tuple) else (w, 0, w.shape[1]) for w in weights]
    spaces += [pl.ANY] * len(weights)
    moved = sum(a.size * a.dtype.itemsize for a in args)
    held = [pltpu.VMEM((w.shape[0], size), w.dtype) for w, _, size in weights]
    if weights:
        held.append(pltpu.SemaphoreType.DMA((len(weights),)))
    count, n_out = len(args), len(jax.tree.leaves(outs))

    def run(*refs):
        n = len(weights)
        if not n:
            return body(*refs)
        far = refs[count : count + n]
        rest = refs[count + n : count + n + n_out]
        near = refs[count + n + n_out : count + n + n_out + n]
        sem = refs[count + n + n_out + n]
        extra = refs[count + n + n_out + n + 1 :]
        views = [f.at[:, at : at + size] for f, (_, at, size) in zip(far, weights)]
        copies = [pltpu.make_async_copy(f, v, sem.at[i]) for i, (f, v) in enumerate(zip(views, near))]
        for copy in copies:
            copy.start()
        body(*refs[:count], list(zip(near, copies)), *rest, *extra)

    return pl.pallas_call(
        run,
        out_shape=outs,
        in_specs=[pl.BlockSpec(memory_space=s) for s in spaces],
        out_specs=jax.tree.map(lambda _: pl.BlockSpec(memory_space=pltpu.VMEM), outs),
        scratch_shapes=[*held, *scratch],
        cost_estimate=pl.CostEstimate(flops=flops, bytes_accessed=moved, transcendentals=0),
        compiler_params=pltpu.CompilerParams(vmem_limit_bytes=limit * 1024 * 1024),
    )(*args, *[w for w, _, _ in weights])


def dot(a, b):
    return jnp.dot(a, b, preferred_element_type=F32)


def dot_t(a, b):
    return lax.dot_general(a, b, (((1,), (1,)), ((), ())), preferred_element_type=F32)


SPANS = ((0, 512), (512, 512), (1024, 256), (1280, 256), (1536, 512))


def block(z, k):
    return pl.ds(pl.multiple_of(lax.rem(z + k, 4) * 512, 512), 512)


def rows_of(index, count):
    return pl.ds(pl.multiple_of(index * count, 16), count)


def times_rows(a, pieces, cols, wait=False):
    total = None
    for (at, size), (p, copy) in zip(SPANS, pieces):
        if wait:
            copy.wait()
        part = dot(a[:, at : at + size], p[:, cols])
        total = part if total is None else total + part
    return total


def mixer_cast_kernel(pieces, copies):
    for i, (w, copy) in enumerate(pieces):
        copy.wait()
        part = w[...].astype(BF)
        for y in range(8):
            copies[y, :, i * 256 : i * 256 + 256] = part


def mlp_cast_kernel(pieces, copies):
    for i, (w, copy) in enumerate(pieces):
        copy.wait()
        part = w[...].astype(BF)
        for y in range(8):
            copies[y, :, i * 768 : i * 768 + 768] = part


def norm_kernel(where, tokens, gain, normed, share):
    z, row = where[0], where[1] * 4 + where[2]
    t = tokens[...].astype(F32)
    scale = lax.rsqrt(jnp.mean(t * t, axis=-1, keepdims=True) + norm_eps)
    for k in range(4):
        at = slice(k * 512, k * 512 + 512)
        normed[:, at] = (tokens[:, block(z, k)].astype(F32) * scale * gain[:, block(z, k)]).astype(BF)
        share[:, at] = tokens[rows_of(row, 48), block(z, k)].astype(F32)


def mixer_kernel(where, normed, cols, taps, pieces, hidden, other, padded):
    value = times_rows(normed, pieces, slice(0, 256), wait=True)
    inner = times_rows(normed, pieces, slice(256, 512))
    gated = inner * value
    padded[0:8, :] = jnp.zeros((8, 256), F32)
    padded[392:400, :] = jnp.zeros((8, 256), F32)
    padded[8:392, :] = gated
    conv = taps[0:1, :] * padded[7:391, :] + taps[1:2, :] * gated + taps[2:3, :] * padded[9:393, :]
    outer = times_rows(normed, pieces, slice(512, 768))
    hidden[...] = (outer * conv * cols[...]).astype(BF)
    theirs = hidden[rows_of(1 - where[1], 192), :]
    for (at, size), (p, _) in zip(SPANS, pieces):
        other[:, at : at + size] = dot_t(theirs, p[:, 768:1024]).astype(BF)


def mix_kernel(where, hidden, got, pieces, mix):
    mine = hidden[rows_of(where[1], 192), :]
    for (at, size), (p, copy) in zip(SPANS, pieces):
        copy.wait()
        part = dot_t(mine, p[...])
        mix[:, at : at + size] = (part + got[:, at : at + size].astype(F32)).astype(BF)


def middle_kernel(where, share, got, cols, gain, middle, copies):
    z = where[0]
    total = got[0].astype(F32) + got[1].astype(F32) + got[2].astype(F32) + got[3].astype(F32)
    mid = share[...] + total * cols[...]
    middle[...] = mid
    scale = lax.rsqrt(jnp.mean(mid * mid, axis=-1, keepdims=True) + norm_eps)
    for k in range(4):
        at = slice(k * 512, k * 512 + 512)
        part = (mid[:, at] * scale * gain[:, block(z, k)]).astype(BF)
        for j in range(4):
            copies[j, :, at] = part


def act_of(rows, pieces, cols, act):
    for _, copy in pieces:
        copy.wait()

    @pl.loop(0, 3)
    def _(i):
        at = pl.ds(pl.multiple_of(i * 256, 256), 256)
        up = times_rows(rows, pieces, at) * cols[:, at]
        act[:, at] = jnp.square(jnp.maximum(up, 0.0)).astype(BF)


def up_kernel(rows, cols, pieces, act):
    act_of(rows, pieces, cols, act)


def up_down_kernel(rows, cols, pieces, other, act):
    act_of(rows, pieces[:5], cols, act)
    for (at, size), (p, copy) in zip(SPANS, pieces[5:]):
        copy.wait()
        other[:, at : at + size] = dot_t(act[...], p[...]).astype(BF)


def down_kernel(act, got, pieces, mlp):
    for (at, size), (p, copy) in zip(SPANS, pieces):
        copy.wait()
        part = dot_t(act[...], p[...])
        mlp[:, at : at + size] = (part + got[:, at : at + size].astype(F32)).astype(BF)


def end_kernel(where, middle, got, cols, copies):
    z = where[0]
    total = got[0].astype(F32) + got[1].astype(F32) + got[2].astype(F32) + got[3].astype(F32)
    end = (middle[...] + total * cols[...]).astype(BF)
    for k in range(4):
        for j in range(4):
            copies[j, :, block(z, k)] = end[:, k * 512 : k * 512 + 512]


def join_kernel(where, mine, theirs, result):
    result[rows_of(where[1], 192), :] = mine[...]
    result[rows_of(1 - where[1], 192), :] = theirs[...]


def body(
    tokens,
    mix_gain,
    value_weight,
    value_scale,
    inner_weight,
    inner_scale,
    outer_weight,
    outer_scale,
    conv_taps,
    out_weight,
    out_scale,
    mlp_gain,
    up_weight,
    up_scale,
    down_weight,
    down_scale,
):
    z = lax.axis_index("zl")
    where = jnp.stack([z, lax.axis_index("c"), lax.axis_index("x")]).astype(jnp.int32)

    vi = jnp.concatenate([value_weight.astype(BF), inner_weight.astype(BF)], axis=1)
    mix_scale = value_scale * inner_scale * outer_scale
    scales = jnp.concatenate([mix_scale, up_scale, out_scale, down_scale])
    scales = everyone(scales[None], FS).reshape(32, 160)
    mix_cols = scales[:, 0:8].reshape(1, 256)
    up_cols = scales[:, 8:32].reshape(1, 768)
    turned = lax.dynamic_slice_in_dim(jnp.concatenate([scales[:, 32:], scales[:24, 32:]], axis=0), z * 8, 32, 0)
    out_cols = turned[:, :64].reshape(1, 2048)
    down_cols = turned[:, 64:].reshape(1, 2048)

    m1 = kernel(
        mixer_cast_kernel,
        SHAPE((8, 64, 1024), BF),
        1_000_000,
        weights=[value_weight, inner_weight, outer_weight, out_weight.T],
        limit=60,
    )
    m1 = spread(m1, "y").reshape(512, 1024)
    m3 = kernel(
        mlp_cast_kernel,
        SHAPE((8, 64, 1536), BF),
        1_000_000,
        weights=[up_weight, down_weight.T],
        limit=60,
    )
    m3 = spread(m3, "y").reshape(512, 1536)
    normed, share = kernel(
        norm_kernel,
        (SHAPE((384, 2048), BF), SHAPE((48, 2048), F32)),
        10_000_000,
        where,
        tokens[0],
        mix_gain[None],
    )
    m1 = [m1, *along_z(m1)]
    up_own, down_own = m3[:, :768], m3[:, 768:]
    up = [(m3, 0, 768), *along_z(up_own)]
    down = [(m3, 768, 768), *along_z(down_own)]

    hidden, mix_other = kernel(
        mixer_kernel,
        (SHAPE((384, 256), BF), SHAPE((192, 2048), BF)),
        1_400_000_000,
        where,
        normed,
        mix_cols,
        conv_taps,
        weights=m1,
        scratch=[pltpu.VMEM((400, 256), F32)],
    )
    got = swap_cores(mix_other)
    out_pieces = [(p, 768, 256) for p in m1]
    mix = kernel(
        mix_kernel, SHAPE((192, 2048), BF), 200_000_000, where, hidden, got, weights=out_pieces
    )
    mix = spread(mix.reshape(4, 48, 2048), "x")
    middle, copies = kernel(
        middle_kernel,
        (SHAPE((48, 2048), F32), SHAPE((4, 48, 2048), BF)),
        2_000_000,
        where,
        share,
        mix,
        out_cols,
        mlp_gain[None],
    )
    own = spread(copies, "x").reshape(192, 2048)
    other = swap_cores(own)
    act = kernel(up_kernel, SHAPE((192, 768), BF), 600_000_000, own, up_cols, weights=up)
    mlp_other = kernel(
        up_down_kernel,
        SHAPE((192, 2048), BF),
        1_200_000_000,
        other,
        up_cols,
        weights=[*up, *down],
        scratch=[pltpu.VMEM((192, 768), BF)],
    )
    got = swap_cores(mlp_other)
    mlp = kernel(down_kernel, SHAPE((192, 2048), BF), 600_000_000, act, got, weights=down)
    mlp = spread(mlp.reshape(4, 48, 2048), "x")
    copies = kernel(end_kernel, SHAPE((4, 48, 2048), BF), 2_000_000, where, middle, mlp, down_cols)
    mine = spread(copies, "x").reshape(192, 2048)
    theirs = swap_cores(mine)
    result = kernel(join_kernel, SHAPE((384, 2048), BF), 1_000_000, where, mine, theirs)
    return result[None]


def solution(mesh):
    fine = Mesh(mesh.devices.reshape(2, 4, 8, 4, 2), ("zh", "zl", "y", "x", "c"))
    rows = P(("zh", "zl", "y"), None, None)
    fs, tp = ("zl", "y"), ("x", "c")
    all_cols = P(tp + fs)
    placed = (
        rows,
        P(),
        P(fs, tp),
        all_cols,
        P(fs, tp),
        all_cols,
        P(fs, tp),
        all_cols,
        P(None, tp),
        P(tp, fs),
        P(fs),
        P(),
        P(fs, tp),
        all_cols,
        P(tp, fs),
        P(fs),
    )
    return jax.shard_map(body, mesh=fine, in_specs=placed, out_specs=rows, check_vma=False)
```

```python
import jax
import jax.numpy as jnp
from jax import lax
from jax.experimental import pallas as pl
from jax.experimental.pallas import tpu as pltpu
from jax.sharding import Mesh, PartitionSpec as P


norm_eps = 1e-06

Z = ("zh", "zl")
FS = ("zl", "y")
BF = jnp.bfloat16
F32 = jnp.float32
SHAPE = jax.ShapeDtypeStruct


def z_shift(a, step):
    return lax.ppermute(a, Z, [(i, (i + step) % 8) for i in range(8)])


def swap_cores(a):
    return lax.ppermute(a, "c", [(0, 1), (1, 0)])


def spread(a, axis):
    return lax.all_to_all(a, axis, 0, 0, tiled=True)


def everyone(a, axis):
    return spread(jnp.broadcast_to(a, (lax.axis_size(axis), *a.shape)), axis)


def along_z(got, far):
    before = z_shift(got, 1)
    after = z_shift(got, -1)
    return [got, after, z_shift(before if far > 0 else after, far), before]


def kernel(body, outs, flops, *args, weights=(), scratch=(), limit=60):
    spaces = [pltpu.SMEM if a.dtype == jnp.int32 else pltpu.VMEM for a in args]
    weights = [w if isinstance(w, tuple) else (w, None, None) for w in weights]
    spaces += [pl.ANY] * len(weights)
    moved = sum(a.size * a.dtype.itemsize for a in args)
    held = [pltpu.VMEM(w.shape if at is None else (w.shape[0], n), w.dtype) for w, at, n in weights]
    if weights:
        held.append(pltpu.SemaphoreType.DMA((len(weights),)))
    count, n_out = len(args), len(jax.tree.leaves(outs))

    def run(*refs):
        many = len(weights)
        if not many:
            return body(*refs)
        end = count + many + n_out
        far, rest = refs[count : count + many], refs[count + many : end]
        near, sem, extra = refs[end : end + many], refs[end + many], refs[end + many + 1 :]
        views = [f if at is None else f.at[:, at : at + n] for f, (_, at, n) in zip(far, weights)]
        copies = [pltpu.make_async_copy(f, v, sem.at[i]) for i, (f, v) in enumerate(zip(views, near))]
        for copy in copies:
            copy.start()
        body(*refs[:count], list(zip(near, copies)), *rest, *extra)

    return pl.pallas_call(
        run,
        out_shape=outs,
        in_specs=[pl.BlockSpec(memory_space=s) for s in spaces],
        out_specs=jax.tree.map(lambda _: pl.BlockSpec(memory_space=pltpu.VMEM), outs),
        scratch_shapes=[*held, *scratch],
        cost_estimate=pl.CostEstimate(flops=flops, bytes_accessed=moved, transcendentals=0),
        compiler_params=pltpu.CompilerParams(vmem_limit_bytes=limit * 1024 * 1024),
    )(*args, *[w for w, _, _ in weights])


def dot(a, b):
    return jnp.dot(a, b, preferred_element_type=F32)


def dot_t(a, b):
    return lax.dot_general(a, b, (((1,), (1,)), ((), ())), preferred_element_type=F32)


SPANS = ((0, 512), (512, 512), (1024, 512), (1536, 512))


def block(z, k):
    return pl.ds(pl.multiple_of(lax.rem(z + k, 4) * 512, 512), 512)


def rows_of(index, count):
    return pl.ds(pl.multiple_of(index * count, 16), count)


def times_rows(a, pieces, cols, wait=False):
    total = None
    for (at, size), (p, copy) in zip(SPANS, pieces):
        if wait:
            copy.wait()
        part = dot(a[:, at : at + size], p[:, cols])
        total = part if total is None else total + part
    return total


def copies_kernel(pieces, copies):
    at = 0
    for w, copy in pieces:
        copy.wait()
        part, width = w[...].astype(BF), w.shape[1]
        for y in range(8):
            copies[y, :, at : at + width] = part
        at += width


def mlp_cast_kernel(pieces, first, second):
    (up, up_copy), (down, down_copy) = pieces
    up_copy.wait()
    first[:, 0:768] = up[...].astype(BF)
    down_copy.wait()
    first[:, 768:1024] = down[:, 0:256].astype(BF)
    second[...] = down[:, 256:768].astype(BF)


def norm_kernel(where, tokens, gain, normed, share):
    z, row = where[0], where[1] * 4 + where[2]
    t = tokens[...].astype(F32)
    scale = lax.rsqrt(jnp.mean(t * t, axis=-1, keepdims=True) + norm_eps)
    for k in range(4):
        at = slice(k * 512, k * 512 + 512)
        normed[:, at] = (tokens[:, block(z, k)].astype(F32) * scale * gain[:, block(z, k)]).astype(BF)
        share[:, at] = tokens[rows_of(row, 48), block(z, k)].astype(F32)


def mixer_kernel(where, normed, cols, taps, pieces, hidden, other, padded):
    vi, oo = pieces[:4], pieces[4:]
    value = times_rows(normed, vi, slice(0, 256), wait=True)
    inner = times_rows(normed, vi, slice(256, 512))
    gated = inner * value
    padded[0:8, :] = jnp.zeros((8, 256), F32)
    padded[392:400, :] = jnp.zeros((8, 256), F32)
    padded[8:392, :] = gated
    conv = taps[0:1, :] * padded[7:391, :] + taps[1:2, :] * gated + taps[2:3, :] * padded[9:393, :]
    outer = times_rows(normed, oo, slice(0, 256), wait=True)
    hidden[...] = (outer * conv * cols[...]).astype(BF)
    theirs = hidden[rows_of(1 - where[1], 192), :]
    for (at, size), (p, _) in zip(SPANS, oo):
        other[:, at : at + size] = dot_t(theirs, p[:, 256:512]).astype(BF)


def mix_kernel(where, hidden, got, pieces, mix):
    mine = hidden[rows_of(where[1], 192), :]
    for (at, size), (p, copy) in zip(SPANS, pieces):
        copy.wait()
        part = dot_t(mine, p[...])
        mix[:, at : at + size] = (part + got[:, at : at + size].astype(F32)).astype(BF)


def middle_kernel(where, share, got, cols, gain, middle, copies):
    z = where[0]
    total = got[0].astype(F32) + got[1].astype(F32) + got[2].astype(F32) + got[3].astype(F32)
    mid = share[...] + total * cols[...]
    middle[...] = mid
    scale = lax.rsqrt(jnp.mean(mid * mid, axis=-1, keepdims=True) + norm_eps)
    for k in range(4):
        at = slice(k * 512, k * 512 + 512)
        part = (mid[:, at] * scale * gain[:, block(z, k)]).astype(BF)
        for j in range(4):
            copies[j, :, at] = part


def act_of(rows, pieces, cols, act, total):
    for k, ((at, size), (p, copy)) in enumerate(zip(SPANS, pieces)):
        copy.wait()
        for n in range(0, 768, 256):
            part = dot(rows[:, at : at + size], p[:, n : n + 256])
            if k:
                part = part + total[:, n : n + 256]
            if k < 3:
                total[:, n : n + 256] = part
            else:
                up = part * cols[:, n : n + 256]
                act[:, n : n + 256] = jnp.square(jnp.maximum(up, 0.0)).astype(BF)


def up_kernel(rows, cols, pieces, act, total):
    act_of(rows, pieces, cols, act, total)


def down_parts(act, pieces):
    first, (second, second_copy) = pieces[:4], pieces[4]
    for k, ((at, size), (p, copy)) in enumerate(zip(SPANS, first)):
        copy.wait()
        if k == 0:
            second_copy.wait()
        part = dot_t(act[:, 0:256], p[...])
        yield slice(at, at + size), part + dot_t(act[:, 256:768], second[:, k].reshape(512, 512))


def up_down_kernel(rows, cols, pieces, other, act, total):
    act_of(rows, pieces[:4], cols, act, total)
    for at, part in down_parts(act, pieces[4:]):
        other[:, at] = part.astype(BF)


def down_kernel(act, got, pieces, mlp):
    for at, part in down_parts(act, pieces):
        mlp[:, at] = (part + got[:, at].astype(F32)).astype(BF)


def end_kernel(where, middle, got, cols, copies):
    z = where[0]
    total = got[0].astype(F32) + got[1].astype(F32) + got[2].astype(F32) + got[3].astype(F32)
    end = (middle[...] + total * cols[...]).astype(BF)
    for k in range(4):
        for j in range(4):
            copies[j, :, block(z, k)] = end[:, k * 512 : k * 512 + 512]


def join_kernel(where, mine, theirs, result):
    result[rows_of(where[1], 192), :] = mine[...]
    result[rows_of(1 - where[1], 192), :] = theirs[...]


def body(
    tokens,
    mix_gain,
    value_weight,
    value_scale,
    inner_weight,
    inner_scale,
    outer_weight,
    outer_scale,
    conv_taps,
    out_weight,
    out_scale,
    mlp_gain,
    up_weight,
    up_scale,
    down_weight,
    down_scale,
):
    z = lax.axis_index("zl")
    where = jnp.stack([z, lax.axis_index("c"), lax.axis_index("x")]).astype(jnp.int32)

    vi = jnp.concatenate([value_weight.astype(BF), inner_weight.astype(BF)], axis=1)
    mix_scale = value_scale * inner_scale * outer_scale
    scales = jnp.concatenate([mix_scale, up_scale, out_scale, down_scale])
    scales = everyone(scales[None], FS).reshape(32, 160)
    mix_cols = scales[:, 0:8].reshape(1, 256)
    up_cols = scales[:, 8:32].reshape(1, 768)
    turned = lax.dynamic_slice_in_dim(jnp.concatenate([scales[:, 32:], scales[:24, 32:]], axis=0), z * 8, 32, 0)
    out_cols = turned[:, :64].reshape(1, 2048)
    down_cols = turned[:, 64:].reshape(1, 2048)

    copies = SHAPE((8, 64, 512), BF)
    vi = kernel(copies_kernel, copies, 1_000_000, weights=[value_weight, inner_weight], limit=60)
    vi = spread(vi, "y").reshape(512, 512)
    oo = kernel(copies_kernel, copies, 1_000_000, weights=[outer_weight, out_weight.T], limit=60)
    oo = spread(oo, "y").reshape(512, 512)
    ud, dn = kernel(
        mlp_cast_kernel,
        (SHAPE((64, 1024), BF), SHAPE((64, 512), BF)),
        1_000_000,
        weights=[up_weight, down_weight.T],
        limit=60,
    )
    ud = lax.all_gather(ud, "y", axis=0, tiled=True)
    dn = [dn, z_shift(dn, -1), z_shift(dn, 2), z_shift(dn, 1)]
    dn = lax.all_gather(jnp.concatenate(dn, axis=0), "y", axis=0, tiled=True)
    dn = dn.reshape(8, 4, 64, 512)
    normed, share = kernel(
        norm_kernel,
        (SHAPE((384, 2048), BF), SHAPE((48, 2048), F32)),
        10_000_000,
        where,
        tokens[0],
        mix_gain[None],
    )
    vi = along_z(vi, 1)
    oo = along_z(oo, -1)
    ud = along_z(ud, 1)
    up = [(p, 0, 768) for p in ud]
    down = [(p, 768, 256) for p in ud] + [dn]

    hidden, mix_other = kernel(
        mixer_kernel,
        (SHAPE((384, 256), BF), SHAPE((192, 2048), BF)),
        1_400_000_000,
        where,
        normed,
        mix_cols,
        conv_taps,
        weights=[*vi, *oo],
        scratch=[pltpu.VMEM((400, 256), F32)],
    )
    got = swap_cores(mix_other)
    out_pieces = [(p, 256, 256) for p in oo]
    mix = kernel(
        mix_kernel, SHAPE((192, 2048), BF), 200_000_000, where, hidden, got, weights=out_pieces
    )
    mix = spread(mix.reshape(4, 48, 2048), "x")
    middle, copies = kernel(
        middle_kernel,
        (SHAPE((48, 2048), F32), SHAPE((4, 48, 2048), BF)),
        2_000_000,
        where,
        share,
        mix,
        out_cols,
        mlp_gain[None],
    )
    own = spread(copies, "x").reshape(192, 2048)
    other = swap_cores(own)
    total = pltpu.VMEM((192, 768), F32)
    act = kernel(
        up_kernel, SHAPE((192, 768), BF), 600_000_000, own, up_cols, weights=up, scratch=[total]
    )
    mlp_other = kernel(
        up_down_kernel,
        SHAPE((192, 2048), BF),
        1_200_000_000,
        other,
        up_cols,
        weights=[*up, *down],
        scratch=[pltpu.VMEM((192, 768), BF), total],
    )
    got = swap_cores(mlp_other)
    mlp = kernel(down_kernel, SHAPE((192, 2048), BF), 600_000_000, act, got, weights=down)
    mlp = spread(mlp.reshape(4, 48, 2048), "x")
    copies = kernel(end_kernel, SHAPE((4, 48, 2048), BF), 2_000_000, where, middle, mlp, down_cols)
    mine = spread(copies, "x").reshape(192, 2048)
    theirs = swap_cores(mine)
    result = kernel(join_kernel, SHAPE((384, 2048), BF), 1_000_000, where, mine, theirs)
    return result[None]


def solution(mesh):
    fine = Mesh(mesh.devices.reshape(2, 4, 8, 4, 2), ("zh", "zl", "y", "x", "c"))
    rows = P(("zh", "zl", "y"), None, None)
    fs, tp = ("zl", "y"), ("x", "c")
    all_cols = P(tp + fs)
    placed = (
        rows,
        P(),
        P(fs, tp),
        all_cols,
        P(fs, tp),
        all_cols,
        P(fs, tp),
        all_cols,
        P(None, tp),
        P(tp, fs),
        P(fs),
        P(),
        P(fs, tp),
        all_cols,
        P(tp, fs),
        P(fs),
    )
    return jax.shard_map(body, mesh=fine, in_specs=placed, out_specs=rows, check_vma=False)
```

```python
import jax
import jax.numpy as jnp
from jax import lax
from jax.experimental import pallas as pl
from jax.experimental.pallas import tpu as pltpu
from jax.sharding import Mesh, PartitionSpec as P


norm_eps = 1e-06

Z = ("zh", "zl")
FS = ("zl", "y")
BF = jnp.bfloat16
F32 = jnp.float32
SHAPE = jax.ShapeDtypeStruct


def z_shift(a, step):
    return lax.ppermute(a, Z, [(i, (i + step) % 8) for i in range(8)])


def swap_cores(a):
    return lax.ppermute(a, "c", [(0, 1), (1, 0)])


def spread(a, axis):
    return lax.all_to_all(a, axis, 0, 0, tiled=True)


def everyone(a, axis):
    return spread(jnp.broadcast_to(a, (lax.axis_size(axis), *a.shape)), axis)


def along_z(got, far):
    before = z_shift(got, 1)
    after = z_shift(got, -1)
    return [got, after, z_shift(before if far > 0 else after, far), before]


def kernel(body, outs, flops, *args, weights=(), scratch=(), fetch=False):
    spaces = [pltpu.SMEM if a.dtype == jnp.int32 else pltpu.VMEM for a in args]
    weights = [w if isinstance(w, tuple) else (w, None, None) for w in weights]
    spaces += [pl.ANY if fetch else pltpu.VMEM] * len(weights)
    moved = sum(a.size * a.dtype.itemsize for a in args)
    held = [pltpu.VMEM(w.shape if at is None else (w.shape[0], n), w.dtype) for w, at, n in weights]
    held = [*held, pltpu.SemaphoreType.DMA((len(weights),))] if fetch else []
    count, n_out = len(args), len(jax.tree.leaves(outs))

    def run(*refs):
        many = len(weights)
        if not many:
            return body(*refs)
        end = count + many + n_out
        far, rest = refs[count : count + many], refs[count + many : end]
        views = [f if at is None else f.at[:, at : at + n] for f, (_, at, n) in zip(far, weights)]
        if not fetch:
            return body(*refs[:count], views, *rest, *refs[end:])
        near, sem, extra = refs[end : end + many], refs[end + many], refs[end + many + 1 :]
        copies = [pltpu.make_async_copy(f, v, sem.at[i]) for i, (f, v) in enumerate(zip(views, near))]
        for copy in copies:
            copy.start()
        body(*refs[:count], list(zip(near, copies)), *rest, *extra)

    return pl.pallas_call(
        run,
        out_shape=outs,
        in_specs=[pl.BlockSpec(memory_space=s) for s in spaces],
        out_specs=jax.tree.map(lambda _: pl.BlockSpec(memory_space=pltpu.VMEM), outs),
        scratch_shapes=[*held, *scratch],
        cost_estimate=pl.CostEstimate(flops=flops, bytes_accessed=moved, transcendentals=0),
        compiler_params=pltpu.CompilerParams(vmem_limit_bytes=(60 if fetch else 20) * 1024 * 1024),
    )(*args, *[w for w, _, _ in weights])


def dot(a, b):
    return jnp.dot(a, b, preferred_element_type=F32)


def dot_t(a, b):
    return lax.dot_general(a, b, (((1,), (1,)), ((), ())), preferred_element_type=F32)


SPANS = ((0, 512), (512, 512), (1024, 512), (1536, 512))


def block(z, k):
    return pl.ds(pl.multiple_of(lax.rem(z + k, 4) * 512, 512), 512)


def rows_of(index, count):
    return pl.ds(pl.multiple_of(index * count, 16), count)


def times_rows(a, pieces, cols):
    total = None
    for (at, size), p in zip(SPANS, pieces):
        part = dot(a[:, at : at + size], p[:, cols])
        total = part if total is None else total + part
    return total


def copies_kernel(pieces, copies):
    at = 0
    for w, copy in pieces:
        copy.wait()
        part, width = w[...].astype(BF), w.shape[1]
        for y in range(8):
            copies[y, :, at : at + width] = part
        at += width


def mlp_cast_kernel(pieces, first, second):
    (up, up_copy), (down, down_copy) = pieces
    up_copy.wait()
    first[:, 0:768] = up[...].astype(BF)
    down_copy.wait()
    first[:, 768:1024] = down[:, 0:256].astype(BF)
    second[...] = down[:, 256:768].astype(BF)


def norm_kernel(where, tokens, gain, normed, share):
    z, row = where[0], where[1] * 4 + where[2]
    t = tokens[...].astype(F32)
    scale = lax.rsqrt(jnp.mean(t * t, axis=-1, keepdims=True) + norm_eps)
    for k in range(4):
        at = slice(k * 512, k * 512 + 512)
        normed[:, at] = (tokens[:, block(z, k)].astype(F32) * scale * gain[:, block(z, k)]).astype(BF)
        share[:, at] = tokens[rows_of(row, 48), block(z, k)].astype(F32)


def conv_kernel(normed, taps, vi, conv, padded):
    value = times_rows(normed, vi, slice(0, 256))
    inner = times_rows(normed, vi, slice(256, 512))
    gated = inner * value
    padded[0:8, :] = jnp.zeros((8, 256), F32)
    padded[392:400, :] = jnp.zeros((8, 256), F32)
    padded[8:392, :] = gated
    conv[...] = taps[0:1, :] * padded[7:391, :] + taps[1:2, :] * gated + taps[2:3, :] * padded[9:393, :]


def hidden_kernel(where, normed, conv, cols, oo, hidden, other):
    outer = times_rows(normed, oo, slice(0, 256))
    hidden[...] = (outer * conv[...] * cols[...]).astype(BF)
    theirs = hidden[rows_of(1 - where[1], 192), :]
    for (at, size), p in zip(SPANS, oo):
        other[:, at : at + size] = dot_t(theirs, p[:, 256:512]).astype(BF)


def mix_kernel(where, hidden, got, oo, mix):
    mine = hidden[rows_of(where[1], 192), :]
    for (at, size), p in zip(SPANS, oo):
        part = dot_t(mine, p[:, 256:512])
        mix[:, at : at + size] = (part + got[:, at : at + size].astype(F32)).astype(BF)


def middle_kernel(where, share, got, cols, gain, middle, copies):
    z = where[0]
    total = got[0].astype(F32) + got[1].astype(F32) + got[2].astype(F32) + got[3].astype(F32)
    mid = share[...] + total * cols[...]
    middle[...] = mid
    scale = lax.rsqrt(jnp.mean(mid * mid, axis=-1, keepdims=True) + norm_eps)
    for k in range(4):
        at = slice(k * 512, k * 512 + 512)
        part = (mid[:, at] * scale * gain[:, block(z, k)]).astype(BF)
        for j in range(4):
            copies[j, :, at] = part


def act_of(rows, ud, cols, act):
    @pl.loop(0, 3)
    def _(i):
        at = pl.ds(pl.multiple_of(i * 256, 256), 256)
        up = times_rows(rows, ud, at) * cols[:, at]
        act[:, at] = jnp.square(jnp.maximum(up, 0.0)).astype(BF)


def up_kernel(rows, cols, ud, act):
    act_of(rows, ud, cols, act)


def down_parts(act, pieces):
    for k, (at, size) in enumerate(SPANS):
        part = dot_t(act[:, 0:256], pieces[k][:, 768:1024])
        yield slice(at, at + size), part + dot_t(act[:, 256:768], pieces[4][:, k].reshape(512, 512))


def up_down_kernel(rows, cols, pieces, other, act):
    act_of(rows, pieces[:4], cols, act)
    for at, part in down_parts(act, pieces):
        other[:, at] = part.astype(BF)


def down_kernel(act, got, pieces, mlp):
    for at, part in down_parts(act, pieces):
        mlp[:, at] = (part + got[:, at].astype(F32)).astype(BF)


def end_kernel(where, middle, got, cols, copies):
    z = where[0]
    total = got[0].astype(F32) + got[1].astype(F32) + got[2].astype(F32) + got[3].astype(F32)
    end = (middle[...] + total * cols[...]).astype(BF)
    for k in range(4):
        for j in range(4):
            copies[j, :, block(z, k)] = end[:, k * 512 : k * 512 + 512]


def join_kernel(where, mine, theirs, result):
    result[rows_of(where[1], 192), :] = mine[...]
    result[rows_of(1 - where[1], 192), :] = theirs[...]


def body(
    tokens,
    mix_gain,
    value_weight,
    value_scale,
    inner_weight,
    inner_scale,
    outer_weight,
    outer_scale,
    conv_taps,
    out_weight,
    out_scale,
    mlp_gain,
    up_weight,
    up_scale,
    down_weight,
    down_scale,
):
    z = lax.axis_index("zl")
    where = jnp.stack([z, lax.axis_index("c"), lax.axis_index("x")]).astype(jnp.int32)

    vi = jnp.concatenate([value_weight.astype(BF), inner_weight.astype(BF)], axis=1)
    mix_scale = value_scale * inner_scale * outer_scale
    scales = jnp.concatenate([mix_scale, up_scale, out_scale, down_scale])
    scales = everyone(scales[None], FS).reshape(32, 160)
    mix_cols = scales[:, 0:8].reshape(1, 256)
    up_cols = scales[:, 8:32].reshape(1, 768)
    turned = lax.dynamic_slice_in_dim(jnp.concatenate([scales[:, 32:], scales[:24, 32:]], axis=0), z * 8, 32, 0)
    out_cols = turned[:, :64].reshape(1, 2048)
    down_cols = turned[:, 64:].reshape(1, 2048)

    copies = SHAPE((8, 64, 512), BF)
    vi = kernel(copies_kernel, copies, 1_000_000, weights=[value_weight, inner_weight], fetch=True)
    vi = spread(vi, "y").reshape(512, 512)
    oo = kernel(copies_kernel, copies, 1_000_000, weights=[outer_weight, out_weight.T], fetch=True)
    oo = spread(oo, "y").reshape(512, 512)
    ud, dn = kernel(
        mlp_cast_kernel,
        (SHAPE((64, 1024), BF), SHAPE((64, 512), BF)),
        1_000_000,
        weights=[up_weight, down_weight.T],
        fetch=True,
    )
    ud = lax.all_gather(ud, "y", axis=0, tiled=True)
    dn = [dn, z_shift(dn, -1), z_shift(dn, 2), z_shift(dn, 1)]
    dn = lax.all_gather(jnp.concatenate(dn, axis=0), "y", axis=0, tiled=True)
    dn = dn.reshape(8, 4, 64, 512)
    normed, share = kernel(
        norm_kernel, (SHAPE((384, 2048), BF), SHAPE((48, 2048), F32)), 10_000_000, where, tokens[0], mix_gain[None]
    )
    vi = along_z(vi, 1)
    oo = along_z(oo, -1)
    ud = along_z(ud, 1)

    conv = kernel(
        conv_kernel,
        SHAPE((384, 256), F32),
        800_000_000,
        normed,
        conv_taps,
        weights=vi,
        scratch=[pltpu.VMEM((400, 256), F32)],
    )
    hidden, mix_other = kernel(
        hidden_kernel,
        (SHAPE((384, 256), BF), SHAPE((192, 2048), BF)),
        600_000_000,
        where,
        normed,
        conv,
        mix_cols,
        weights=oo,
    )
    got = swap_cores(mix_other)
    mix = kernel(mix_kernel, SHAPE((192, 2048), BF), 200_000_000, where, hidden, got, weights=oo)
    mix = spread(mix.reshape(4, 48, 2048), "x")
    middle, copies = kernel(
        middle_kernel,
        (SHAPE((48, 2048), F32), SHAPE((4, 48, 2048), BF)),
        2_000_000,
        where,
        share,
        mix,
        out_cols,
        mlp_gain[None],
    )
    own = spread(copies, "x").reshape(192, 2048)
    other = swap_cores(own)
    act = kernel(up_kernel, SHAPE((192, 768), BF), 600_000_000, own, up_cols, weights=ud)
    mlp_other = kernel(
        up_down_kernel,
        SHAPE((192, 2048), BF),
        1_200_000_000,
        other,
        up_cols,
        weights=[*ud, dn],
        scratch=[pltpu.VMEM((192, 768), BF)],
    )
    got = swap_cores(mlp_other)
    mlp = kernel(down_kernel, SHAPE((192, 2048), BF), 600_000_000, act, got, weights=[*ud, dn])
    mlp = spread(mlp.reshape(4, 48, 2048), "x")
    copies = kernel(end_kernel, SHAPE((4, 48, 2048), BF), 2_000_000, where, middle, mlp, down_cols)
    mine = spread(copies, "x").reshape(192, 2048)
    theirs = swap_cores(mine)
    result = kernel(join_kernel, SHAPE((384, 2048), BF), 1_000_000, where, mine, theirs)
    return result[None]


def solution(mesh):
    fine = Mesh(mesh.devices.reshape(2, 4, 8, 4, 2), ("zh", "zl", "y", "x", "c"))
    rows = P(("zh", "zl", "y"), None, None)
    fs, tp = ("zl", "y"), ("x", "c")
    all_cols = P(tp + fs)
    placed = (
        rows,
        P(),
        P(fs, tp),
        all_cols,
        P(fs, tp),
        all_cols,
        P(fs, tp),
        all_cols,
        P(None, tp),
        P(tp, fs),
        P(fs),
        P(),
        P(fs, tp),
        all_cols,
        P(tp, fs),
        P(fs),
    )
    return jax.shard_map(body, mesh=fine, in_specs=placed, out_specs=rows, check_vma=False)
```

```python
import jax
import jax.numpy as jnp
from jax import lax
from jax.experimental import pallas as pl
from jax.experimental.pallas import tpu as pltpu
from jax.sharding import Mesh, PartitionSpec as P


norm_eps = 1e-06

Z = ("zh", "zl")
BF = jnp.bfloat16
F32 = jnp.float32
SHAPE = jax.ShapeDtypeStruct


def z_shift(a, step):
    return lax.ppermute(a, Z, [(i, (i + step) % 8) for i in range(8)])


def swap_cores(a):
    return lax.ppermute(a, "c", [(0, 1), (1, 0)])


def spread(a, axis):
    return lax.all_to_all(a, axis, 0, 0, tiled=True)


def along_z(got, far):
    before = z_shift(got, 1)
    after = z_shift(got, -1)
    return [got, after, z_shift(before if far > 0 else after, far), before]


def kernel(body, outs, flops, *args, weights=(), scratch=(), fetch=False):
    spaces = [pltpu.SMEM if a.dtype == jnp.int32 else pltpu.VMEM for a in args]
    weights = [w if isinstance(w, tuple) else (w, None, None) for w in weights]
    spaces += [pl.ANY if fetch else pltpu.VMEM] * len(weights)
    moved = sum(a.size * a.dtype.itemsize for a in args)
    held = [pltpu.VMEM(w.shape if at is None else (w.shape[0], n), w.dtype) for w, at, n in weights]
    held = [*held, pltpu.SemaphoreType.DMA((len(weights),))] if fetch else []
    count, n_out = len(args), len(jax.tree.leaves(outs))

    def run(*refs):
        many = len(weights)
        if not many:
            return body(*refs)
        end = count + many + n_out
        far, rest = refs[count : count + many], refs[count + many : end]
        views = [f if at is None else f.at[:, at : at + n] for f, (_, at, n) in zip(far, weights)]
        if not fetch:
            return body(*refs[:count], views, *rest, *refs[end:])
        near, sem, extra = refs[end : end + many], refs[end + many], refs[end + many + 1 :]
        copies = [pltpu.make_async_copy(f, v, sem.at[i]) for i, (f, v) in enumerate(zip(views, near))]
        for copy in copies:
            copy.start()
        body(*refs[:count], list(zip(near, copies)), *rest, *extra)

    return pl.pallas_call(
        run,
        out_shape=outs,
        in_specs=[pl.BlockSpec(memory_space=s) for s in spaces],
        out_specs=jax.tree.map(lambda _: pl.BlockSpec(memory_space=pltpu.VMEM), outs),
        scratch_shapes=[*held, *scratch],
        cost_estimate=pl.CostEstimate(flops=flops, bytes_accessed=moved, transcendentals=0),
        compiler_params=pltpu.CompilerParams(vmem_limit_bytes=(60 if fetch else 20) * 1024 * 1024),
    )(*args, *[w for w, _, _ in weights])


def dot(a, b):
    return jnp.dot(a, b, preferred_element_type=F32)


def dot_t(a, b):
    return lax.dot_general(a, b, (((1,), (1,)), ((), ())), preferred_element_type=F32)


SPANS = ((0, 512), (512, 512), (1024, 512), (1536, 512))


def block(z, k):
    return pl.ds(pl.multiple_of(lax.rem(z + k, 4) * 512, 512), 512)


def rows_of(index, count):
    return pl.ds(pl.multiple_of(index * count, 16), count)


def times_rows(a, pieces, cols):
    total = None
    for (at, size), p in zip(SPANS, pieces):
        part = dot(a[:, at : at + size], p[:, cols])
        total = part if total is None else total + part
    return total


def copies_kernel(pieces, copies):
    at = 0
    for w, copy in pieces:
        copy.wait()
        part, width = w[...].astype(BF), w.shape[1]
        for y in range(8):
            copies[y, :, at : at + width] = part
        at += width


def copies_scales_kernel(scales, pieces, copies):
    copies_kernel(pieces, copies)
    left = scales[...]
    for i in range(3):
        part = left.astype(BF)
        left = left - part.astype(F32)
        for y in range(8):
            copies[y, i * 16 : i * 16 + 16, 512:640] = part
    for y in range(8):
        copies[y, 48:64, 512:640] = jnp.zeros((16, 128), BF)


def read_scales(oo, mix_cols, up_cols, out_cols, down_cols):
    total = None
    for k in range(4):
        parts = oo[k][:, 512:640].astype(F32).reshape(8, 64, 128).sum(axis=0)
        rows = parts[0:16] + parts[16:32] + parts[32:48]
        total = rows if total is None else total + rows
        for i in range(4):
            at = slice(k * 512 + i * 128, k * 512 + i * 128 + 128)
            out_cols[:, at] = rows[8 + i : 9 + i]
            down_cols[:, at] = rows[12 + i : 13 + i]
    for i in range(2):
        mix_cols[:, i * 128 : i * 128 + 128] = total[i : i + 1]
    for i in range(6):
        up_cols[:, i * 128 : i * 128 + 128] = total[2 + i : 3 + i]


def mlp_cast_kernel(pieces, first, second):
    (up, up_copy), (down, down_copy) = pieces
    up_copy.wait()
    first[:, 0:768] = up[...].astype(BF)
    down_copy.wait()
    first[:, 768:1024] = down[:, 0:256].astype(BF)
    second[...] = down[:, 256:768].astype(BF)


def norm_kernel(where, tokens, gain, normed, share):
    z, row = where[0], where[1] * 4 + where[2]
    t = tokens[...].astype(F32)
    scale = lax.rsqrt(jnp.mean(t * t, axis=-1, keepdims=True) + norm_eps)
    for k in range(4):
        at = slice(k * 512, k * 512 + 512)
        normed[:, at] = (tokens[:, block(z, k)].astype(F32) * scale * gain[:, block(z, k)]).astype(BF)
        share[:, at] = tokens[rows_of(row, 48), block(z, k)].astype(F32)


def conv_kernel(normed, taps, vi, conv, padded):
    value = times_rows(normed, vi, slice(0, 256))
    inner = times_rows(normed, vi, slice(256, 512))
    gated = inner * value
    padded[0:8, :] = jnp.zeros((8, 256), F32)
    padded[392:400, :] = jnp.zeros((8, 256), F32)
    padded[8:392, :] = gated
    conv[...] = taps[0:1, :] * padded[7:391, :] + taps[1:2, :] * gated + taps[2:3, :] * padded[9:393, :]


def hidden_kernel(where, normed, conv, oo, hidden, other, up_cols, out_cols, down_cols, cols):
    read_scales(oo, cols, up_cols, out_cols, down_cols)
    outer = times_rows(normed, oo, slice(0, 256))
    hidden[...] = (outer * conv[...] * cols[...]).astype(BF)
    theirs = hidden[rows_of(1 - where[1], 192), :]
    for (at, size), p in zip(SPANS, oo):
        other[:, at : at + size] = dot_t(theirs, p[:, 256:512]).astype(BF)


def mix_kernel(where, hidden, got, oo, mix):
    mine = hidden[rows_of(where[1], 192), :]
    for (at, size), p in zip(SPANS, oo):
        part = dot_t(mine, p[:, 256:512])
        mix[:, at : at + size] = (part + got[:, at : at + size].astype(F32)).astype(BF)


def middle_kernel(where, share, got, cols, gain, middle, copies):
    z = where[0]
    total = got[0].astype(F32) + got[1].astype(F32) + got[2].astype(F32) + got[3].astype(F32)
    mid = share[...] + total * cols[...]
    middle[...] = mid
    scale = lax.rsqrt(jnp.mean(mid * mid, axis=-1, keepdims=True) + norm_eps)
    for k in range(4):
        at = slice(k * 512, k * 512 + 512)
        part = (mid[:, at] * scale * gain[:, block(z, k)]).astype(BF)
        for j in range(4):
            copies[j, :, at] = part


def act_of(rows, ud, cols, act):
    @pl.loop(0, 3)
    def _(i):
        at = pl.ds(pl.multiple_of(i * 256, 256), 256)
        up = times_rows(rows, ud, at) * cols[:, at]
        act[:, at] = jnp.square(jnp.maximum(up, 0.0)).astype(BF)


def up_kernel(rows, cols, ud, act):
    act_of(rows, ud, cols, act)


def down_parts(act, pieces):
    for k, (at, size) in enumerate(SPANS):
        part = dot_t(act[:, 0:256], pieces[k][:, 768:1024])
        yield slice(at, at + size), part + dot_t(act[:, 256:768], pieces[4][:, k].reshape(512, 512))


def up_down_kernel(rows, cols, pieces, other, act):
    act_of(rows, pieces[:4], cols, act)
    for at, part in down_parts(act, pieces):
        other[:, at] = part.astype(BF)


def down_kernel(act, got, pieces, mlp):
    for at, part in down_parts(act, pieces):
        mlp[:, at] = (part + got[:, at].astype(F32)).astype(BF)


def end_kernel(where, middle, got, cols, copies):
    z = where[0]
    total = got[0].astype(F32) + got[1].astype(F32) + got[2].astype(F32) + got[3].astype(F32)
    end = (middle[...] + total * cols[...]).astype(BF)
    for k in range(4):
        for j in range(4):
            copies[j, :, block(z, k)] = end[:, k * 512 : k * 512 + 512]


def join_kernel(where, mine, theirs, result):
    result[rows_of(where[1], 192), :] = mine[...]
    result[rows_of(1 - where[1], 192), :] = theirs[...]


def body(
    tokens,
    mix_gain,
    value_weight,
    value_scale,
    inner_weight,
    inner_scale,
    outer_weight,
    outer_scale,
    conv_taps,
    out_weight,
    out_scale,
    mlp_gain,
    up_weight,
    up_scale,
    down_weight,
    down_scale,
):
    z = lax.axis_index("zl")
    where = jnp.stack([z, lax.axis_index("c"), lax.axis_index("x")]).astype(jnp.int32)

    vi = jnp.concatenate([value_weight.astype(BF), inner_weight.astype(BF)], axis=1)
    mix_scale = value_scale * inner_scale * outer_scale
    y = lax.axis_index("y")
    scales = jnp.zeros(2048, F32)
    for v, at in (
        (mix_scale, (z * 8 + y) * 8),
        (up_scale, 256 + (z * 8 + y) * 24),
        (out_scale, 1024 + y * 64),
        (down_scale, 1536 + y * 64),
    ):
        scales = lax.dynamic_update_slice_in_dim(scales, v, at, 0)

    copies = SHAPE((8, 64, 512), BF)
    vi = kernel(copies_kernel, copies, 1_000_000, weights=[value_weight, inner_weight], fetch=True)
    vi = spread(vi, "y").reshape(512, 512)
    oo = kernel(
        copies_scales_kernel,
        SHAPE((8, 64, 640), BF),
        1_000_000,
        scales.reshape(16, 128),
        weights=[outer_weight, out_weight.T],
        fetch=True,
    )
    oo = spread(oo, "y").reshape(512, 640)
    ud, dn = kernel(
        mlp_cast_kernel,
        (SHAPE((64, 1024), BF), SHAPE((64, 512), BF)),
        1_000_000,
        weights=[up_weight, down_weight.T],
        fetch=True,
    )
    ud = lax.all_gather(ud, "y", axis=0, tiled=True)
    dn = [dn, z_shift(dn, -1), z_shift(dn, 2), z_shift(dn, 1)]
    dn = lax.all_gather(jnp.concatenate(dn, axis=0), "y", axis=0, tiled=True)
    dn = dn.reshape(8, 4, 64, 512)
    normed, share = kernel(
        norm_kernel,
        (SHAPE((384, 2048), BF), SHAPE((48, 2048), F32)),
        10_000_000,
        where,
        tokens[0],
        mix_gain[None],
    )
    vi = along_z(vi, 1)
    oo = along_z(oo, -1)
    ud = along_z(ud, 1)

    conv = kernel(
        conv_kernel,
        SHAPE((384, 256), F32),
        800_000_000,
        normed,
        conv_taps,
        weights=vi,
        scratch=[pltpu.VMEM((400, 256), F32)],
    )
    wide = SHAPE((1, 2048), F32)
    hidden, mix_other, up_cols, out_cols, down_cols = kernel(
        hidden_kernel,
        (SHAPE((384, 256), BF), SHAPE((192, 2048), BF), SHAPE((1, 768), F32), wide, wide),
        600_000_000,
        where,
        normed,
        conv,
        weights=oo,
        scratch=[pltpu.VMEM((1, 256), F32)],
    )
    got = swap_cores(mix_other)
    mix = kernel(mix_kernel, SHAPE((192, 2048), BF), 200_000_000, where, hidden, got, weights=oo)
    mix = spread(mix.reshape(4, 48, 2048), "x")
    middle, copies = kernel(
        middle_kernel,
        (SHAPE((48, 2048), F32), SHAPE((4, 48, 2048), BF)),
        2_000_000,
        where,
        share,
        mix,
        out_cols,
        mlp_gain[None],
    )
    own = spread(copies, "x").reshape(192, 2048)
    other = swap_cores(own)
    act = kernel(up_kernel, SHAPE((192, 768), BF), 600_000_000, own, up_cols, weights=ud)
    mlp_other = kernel(
        up_down_kernel,
        SHAPE((192, 2048), BF),
        1_200_000_000,
        other,
        up_cols,
        weights=[*ud, dn],
        scratch=[pltpu.VMEM((192, 768), BF)],
    )
    got = swap_cores(mlp_other)
    mlp = kernel(down_kernel, SHAPE((192, 2048), BF), 600_000_000, act, got, weights=[*ud, dn])
    mlp = spread(mlp.reshape(4, 48, 2048), "x")
    copies = kernel(end_kernel, SHAPE((4, 48, 2048), BF), 2_000_000, where, middle, mlp, down_cols)
    mine = spread(copies, "x").reshape(192, 2048)
    theirs = swap_cores(mine)
    result = kernel(join_kernel, SHAPE((384, 2048), BF), 1_000_000, where, mine, theirs)
    return result[None]


def solution(mesh):
    fine = Mesh(mesh.devices.reshape(2, 4, 8, 4, 2), ("zh", "zl", "y", "x", "c"))
    rows = P(("zh", "zl", "y"), None, None)
    fs, tp = ("zl", "y"), ("x", "c")
    all_cols = P(tp + fs)
    placed = (
        rows,
        P(),
        P(fs, tp),
        all_cols,
        P(fs, tp),
        all_cols,
        P(fs, tp),
        all_cols,
        P(None, tp),
        P(tp, fs),
        P(fs),
        P(),
        P(fs, tp),
        all_cols,
        P(tp, fs),
        P(fs),
    )
    return jax.shard_map(body, mesh=fine, in_specs=placed, out_specs=rows, check_vma=False)
```

```python
import jax
import jax.numpy as jnp
from jax import lax
from jax.experimental import pallas as pl
from jax.experimental.pallas import tpu as pltpu
from jax.sharding import Mesh, PartitionSpec as P


norm_eps = 1e-06

Z = ("zh", "zl")
BF = jnp.bfloat16
F32 = jnp.float32
SHAPE = jax.ShapeDtypeStruct


def z_shift(a, step):
    return lax.ppermute(a, Z, [(i, (i + step) % 8) for i in range(8)])


def swap_cores(a):
    return lax.ppermute(a, "c", [(0, 1), (1, 0)])


def spread(a, axis):
    return lax.all_to_all(a, axis, 0, 0, tiled=True)


def along_z(got, far):
    before = z_shift(got, 1)
    after = z_shift(got, -1)
    return [got, after, z_shift(before if far > 0 else after, far), before]


def z_then_y(a):
    near = [z_shift(a, step) for step in (-1, 2, 1)]
    width = a.shape[1]
    stacked = kernel(stack_kernel, SHAPE((256, width), BF), 1_000_000, a, *near)
    return lax.all_gather(stacked, "y", axis=0, tiled=True).reshape(8, 4, 64, width)


def kernel(body, outs, flops, *args, weights=(), scratch=(), fetch=False):
    spaces = [pltpu.SMEM if a.dtype == jnp.int32 else pltpu.VMEM for a in args]
    weights = [w if isinstance(w, tuple) else (w, None, None) for w in weights]
    spaces += [pl.ANY if fetch else pltpu.VMEM] * len(weights)
    moved = sum(a.size * a.dtype.itemsize for a in args)
    held = [pltpu.VMEM(w.shape if at is None else (w.shape[0], n), w.dtype) for w, at, n in weights]
    held = [*held, pltpu.SemaphoreType.DMA((len(weights),))] if fetch else []
    count, n_out = len(args), len(jax.tree.leaves(outs))

    def run(*refs):
        many = len(weights)
        if not many:
            return body(*refs)
        end = count + many + n_out
        far, rest = refs[count : count + many], refs[count + many : end]
        views = [f if at is None else f.at[:, at : at + n] for f, (_, at, n) in zip(far, weights)]
        if not fetch:
            return body(*refs[:count], views, *rest, *refs[end:])
        near, sem, extra = refs[end : end + many], refs[end + many], refs[end + many + 1 :]
        copies = [pltpu.make_async_copy(f, v, sem.at[i]) for i, (f, v) in enumerate(zip(views, near))]
        for copy in copies:
            copy.start()
        body(*refs[:count], list(zip(near, copies)), *rest, *extra)

    return pl.pallas_call(
        run,
        out_shape=outs,
        in_specs=[pl.BlockSpec(memory_space=s) for s in spaces],
        out_specs=jax.tree.map(lambda _: pl.BlockSpec(memory_space=pltpu.VMEM), outs),
        scratch_shapes=[*held, *scratch],
        cost_estimate=pl.CostEstimate(flops=flops, bytes_accessed=moved, transcendentals=0),
        compiler_params=pltpu.CompilerParams(vmem_limit_bytes=(60 if fetch else 20) * 1024 * 1024),
    )(*args, *[w for w, _, _ in weights])


def dot(a, b):
    return jnp.dot(a, b, preferred_element_type=F32)


def dot_t(a, b):
    return lax.dot_general(a, b, (((1,), (1,)), ((), ())), preferred_element_type=F32)


SPANS = ((0, 512), (512, 512), (1024, 512), (1536, 512))


def block(z, k):
    return pl.ds(pl.multiple_of(lax.rem(z + k, 4) * 512, 512), 512)


def rows_of(index, count):
    return pl.ds(pl.multiple_of(index * count, 16), count)


def times_rows(a, pieces, cols):
    total = None
    for (at, size), p in zip(SPANS, pieces):
        part = dot(a[:, at : at + size], p[:, cols])
        total = part if total is None else total + part
    return total


def copies_kernel(pieces, copies):
    at = 0
    for w, copy in pieces:
        copy.wait()
        part, width = w[...].astype(BF), w.shape[1]
        for y in range(8):
            copies[y, :, at : at + width] = part
        at += width


def copies_scales_kernel(scales, pieces, copies):
    copies_kernel(pieces, copies)
    left = scales[...]
    for i in range(3):
        part = left.astype(BF)
        left = left - part.astype(F32)
        for y in range(8):
            copies[y, i * 16 : i * 16 + 16, 512:640] = part
    for y in range(8):
        copies[y, 48:64, 512:640] = jnp.zeros((16, 128), BF)


def read_scales(vi, mix_cols, up_cols, out_cols, down_cols):
    total = None
    for k in range(4):
        parts = vi[k][:, 512:640].astype(F32).reshape(8, 64, 128).sum(axis=0)
        rows = parts[0:16] + parts[16:32] + parts[32:48]
        total = rows if total is None else total + rows
        for i in range(4):
            at = slice(k * 512 + i * 128, k * 512 + i * 128 + 128)
            out_cols[:, at] = rows[8 + i : 9 + i]
            down_cols[:, at] = rows[12 + i : 13 + i]
    for i in range(2):
        mix_cols[:, i * 128 : i * 128 + 128] = total[i : i + 1]
    for i in range(6):
        up_cols[:, i * 128 : i * 128 + 128] = total[2 + i : 3 + i]


def mlp_cast_kernel(pieces, up, down):
    copies_kernel(pieces[:1], up)
    w, copy = pieces[1]
    copy.wait()
    down[...] = w[...].astype(BF)


def side_kernel(pieces, both):
    at = 0
    for w, copy in pieces:
        copy.wait()
        both[:, at : at + w.shape[1]] = w[...].astype(BF)
        at += w.shape[1]


def stack_kernel(first, second, third, fourth, stacked):
    for i, w in enumerate((first, second, third, fourth)):
        stacked[i * 64 : i * 64 + 64, :] = w[...]


def norm_kernel(where, tokens, gain, normed, share):
    z, row = where[0], where[1] * 4 + where[2]
    t = tokens[...].astype(F32)
    scale = lax.rsqrt(jnp.mean(t * t, axis=-1, keepdims=True) + norm_eps)
    for k in range(4):
        at = slice(k * 512, k * 512 + 512)
        normed[:, at] = (tokens[:, block(z, k)].astype(F32) * scale * gain[:, block(z, k)]).astype(BF)
        share[:, at] = tokens[rows_of(row, 48), block(z, k)].astype(F32)


def conv_kernel(normed, taps, vi, conv, cols, up_cols, out_cols, down_cols, padded):
    read_scales(vi, cols, up_cols, out_cols, down_cols)
    value = times_rows(normed, vi, slice(0, 256))
    inner = times_rows(normed, vi, slice(256, 512))
    gated = inner * value
    padded[0:8, :] = jnp.zeros((8, 256), F32)
    padded[392:400, :] = jnp.zeros((8, 256), F32)
    padded[8:392, :] = gated
    mixed = taps[0:1, :] * padded[7:391, :] + taps[1:2, :] * gated + taps[2:3, :] * padded[9:393, :]
    conv[...] = mixed * cols[...]


def z_piece(w, k, at, n):
    return w[:, k, :, at : at + n].reshape(512, n)


def hidden_kernel(where, normed, conv, oo, hidden, other):
    outer = times_rows(normed, [z_piece(oo[0], k, 0, 256) for k in range(4)], slice(0, 256))
    hidden[...] = (outer * conv[...]).astype(BF)
    theirs = hidden[rows_of(1 - where[1], 192), :]
    for k, (at, size) in enumerate(SPANS):
        other[:, at : at + size] = dot_t(theirs, z_piece(oo[0], k, 256, 256)).astype(BF)


def mix_kernel(where, hidden, got, oo, mix):
    mine = hidden[rows_of(where[1], 192), :]
    for k, (at, size) in enumerate(SPANS):
        part = dot_t(mine, z_piece(oo[0], k, 256, 256))
        mix[:, at : at + size] = (part + got[:, at : at + size].astype(F32)).astype(BF)


def middle_kernel(where, share, got, cols, gain, middle, copies):
    z = where[0]
    total = got[0].astype(F32) + got[1].astype(F32) + got[2].astype(F32) + got[3].astype(F32)
    mid = share[...] + total * cols[...]
    middle[...] = mid
    scale = lax.rsqrt(jnp.mean(mid * mid, axis=-1, keepdims=True) + norm_eps)
    for k in range(4):
        at = slice(k * 512, k * 512 + 512)
        part = (mid[:, at] * scale * gain[:, block(z, k)]).astype(BF)
        for j in range(4):
            copies[j, :, at] = part


def act_of(rows, ud, cols, act):
    @pl.loop(0, 3)
    def _(i):
        at = pl.ds(pl.multiple_of(i * 256, 256), 256)
        up = times_rows(rows, ud, at) * cols[:, at]
        act[:, at] = jnp.square(jnp.maximum(up, 0.0)).astype(BF)


def up_kernel(rows, cols, ud, act):
    act_of(rows, ud, cols, act)


def down_parts(act, down):
    for k, (at, size) in enumerate(SPANS):
        yield slice(at, at + size), dot_t(act[...], z_piece(down, k, 0, 768))


def up_down_kernel(rows, cols, pieces, other, act):
    act_of(rows, pieces[:4], cols, act)
    for at, part in down_parts(act, pieces[4]):
        other[:, at] = part.astype(BF)


def down_kernel(act, got, pieces, mlp):
    for at, part in down_parts(act, pieces[0]):
        mlp[:, at] = (part + got[:, at].astype(F32)).astype(BF)


def end_kernel(where, middle, got, cols, copies):
    z = where[0]
    total = got[0].astype(F32) + got[1].astype(F32) + got[2].astype(F32) + got[3].astype(F32)
    end = (middle[...] + total * cols[...]).astype(BF)
    for k in range(4):
        for j in range(4):
            copies[j, :, block(z, k)] = end[:, k * 512 : k * 512 + 512]


def join_kernel(where, mine, theirs, result):
    result[rows_of(where[1], 192), :] = mine[...]
    result[rows_of(1 - where[1], 192), :] = theirs[...]


def body(
    tokens,
    mix_gain,
    value_weight,
    value_scale,
    inner_weight,
    inner_scale,
    outer_weight,
    outer_scale,
    conv_taps,
    out_weight,
    out_scale,
    mlp_gain,
    up_weight,
    up_scale,
    down_weight,
    down_scale,
):
    z = lax.axis_index("zl")
    where = jnp.stack([z, lax.axis_index("c"), lax.axis_index("x")]).astype(jnp.int32)

    vi = jnp.concatenate([value_weight.astype(BF), inner_weight.astype(BF)], axis=1)
    mix_scale = value_scale * inner_scale * outer_scale
    y = lax.axis_index("y")
    scales = jnp.zeros(2048, F32)
    for v, at in (
        (mix_scale, (z * 8 + y) * 8),
        (up_scale, 256 + (z * 8 + y) * 24),
        (out_scale, 1024 + y * 64),
        (down_scale, 1536 + y * 64),
    ):
        scales = lax.dynamic_update_slice_in_dim(scales, v, at, 0)

    vi = kernel(
        copies_scales_kernel,
        SHAPE((8, 64, 640), BF),
        1_000_000,
        scales.reshape(16, 128),
        weights=[value_weight, inner_weight],
        fetch=True,
    )
    vi = spread(vi, "y").reshape(512, 640)
    oo = kernel(
        side_kernel,
        SHAPE((64, 512), BF),
        1_000_000,
        weights=[outer_weight, out_weight.T],
        fetch=True,
    )
    up, dn = kernel(
        mlp_cast_kernel,
        (SHAPE((8, 64, 768), BF), SHAPE((64, 768), BF)),
        1_000_000,
        weights=[up_weight, down_weight.T],
        fetch=True,
    )
    oo = z_then_y(oo)
    up = spread(up, "y").reshape(512, 768)
    dn = z_then_y(dn)
    normed, share = kernel(
        norm_kernel,
        (SHAPE((384, 2048), BF), SHAPE((48, 2048), F32)),
        10_000_000,
        where,
        tokens[0],
        mix_gain[None],
    )
    vi = along_z(vi, 1)
    up = along_z(up, 1)

    wide = SHAPE((1, 2048), F32)
    conv, _, up_cols, out_cols, down_cols = kernel(
        conv_kernel,
        (SHAPE((384, 256), F32), SHAPE((1, 256), F32), SHAPE((1, 768), F32), wide, wide),
        800_000_000,
        normed,
        conv_taps,
        weights=vi,
        scratch=[pltpu.VMEM((400, 256), F32)],
    )
    hidden, mix_other = kernel(
        hidden_kernel,
        (SHAPE((384, 256), BF), SHAPE((192, 2048), BF)),
        600_000_000,
        where,
        normed,
        conv,
        weights=[oo],
    )
    got = swap_cores(mix_other)
    mix = kernel(mix_kernel, SHAPE((192, 2048), BF), 200_000_000, where, hidden, got, weights=[oo])
    mix = spread(mix.reshape(4, 48, 2048), "x")
    middle, copies = kernel(
        middle_kernel,
        (SHAPE((48, 2048), F32), SHAPE((4, 48, 2048), BF)),
        2_000_000,
        where,
        share,
        mix,
        out_cols,
        mlp_gain[None],
    )
    own = spread(copies, "x").reshape(192, 2048)
    other = swap_cores(own)
    act = kernel(up_kernel, SHAPE((192, 768), BF), 600_000_000, own, up_cols, weights=up)
    mlp_other = kernel(
        up_down_kernel,
        SHAPE((192, 2048), BF),
        1_200_000_000,
        other,
        up_cols,
        weights=[*up, dn],
        scratch=[pltpu.VMEM((192, 768), BF)],
    )
    got = swap_cores(mlp_other)
    mlp = kernel(down_kernel, SHAPE((192, 2048), BF), 600_000_000, act, got, weights=[dn])
    mlp = spread(mlp.reshape(4, 48, 2048), "x")
    copies = kernel(end_kernel, SHAPE((4, 48, 2048), BF), 2_000_000, where, middle, mlp, down_cols)
    mine = spread(copies, "x").reshape(192, 2048)
    theirs = swap_cores(mine)
    result = kernel(join_kernel, SHAPE((384, 2048), BF), 1_000_000, where, mine, theirs)
    return result[None]


def solution(mesh):
    fine = Mesh(mesh.devices.reshape(2, 4, 8, 4, 2), ("zh", "zl", "y", "x", "c"))
    rows = P(("zh", "zl", "y"), None, None)
    fs, tp = ("zl", "y"), ("x", "c")
    all_cols = P(tp + fs)
    placed = (
        rows,
        P(),
        P(fs, tp),
        all_cols,
        P(fs, tp),
        all_cols,
        P(fs, tp),
        all_cols,
        P(None, tp),
        P(tp, fs),
        P(fs),
        P(),
        P(fs, tp),
        all_cols,
        P(tp, fs),
        P(fs),
    )
    return jax.shard_map(body, mesh=fine, in_specs=placed, out_specs=rows, check_vma=False)
```

```python
import jax
import jax.numpy as jnp
from jax import lax
from jax.experimental import pallas as pl
from jax.experimental.pallas import tpu as pltpu
from jax.sharding import Mesh, PartitionSpec as P


norm_eps = 1e-06

Z = ("zh", "zl")
BF = jnp.bfloat16
F32 = jnp.float32
SHAPE = jax.ShapeDtypeStruct


def z_shift(a, step):
    return lax.ppermute(a, Z, [(i, (i + step) % 8) for i in range(8)])


def swap_cores(a):
    return lax.ppermute(a, "c", [(0, 1), (1, 0)])


def spread(a, axis):
    return lax.all_to_all(a, axis, 0, 0, tiled=True)


def along_z(got, far):
    before = z_shift(got, 1)
    after = z_shift(got, -1)
    return [got, after, z_shift(before if far > 0 else after, far), before]


def z_then_y(a, far):
    near = [z_shift(a, step) for step in (-1, far, 1)]
    width = a.shape[1]
    stacked = kernel(stack_kernel, SHAPE((256, width), BF), 1_000_000, a, *near)
    return lax.all_gather(stacked, "y", axis=0, tiled=True).reshape(8, 4, 64, width)


def kernel(body, outs, flops, *args, weights=(), late=(), scratch=()):
    spaces = [pltpu.SMEM if a.dtype == jnp.int32 else pltpu.VMEM for a in (*args, *weights)]
    spaces += [pl.ANY] * len(late)
    moved = sum(a.size * a.dtype.itemsize for a in (*args, *weights, *late))
    held = [pltpu.VMEM(w.shape, w.dtype) for w in late]
    held += [pltpu.SemaphoreType.DMA((len(late),))] if late else []
    count, n_out = len(args), len(jax.tree.leaves(outs))

    def run(*refs):
        given, first, end = list(refs[:count]), count + len(weights), count + len(weights) + len(late)
        if weights:
            given.append(list(refs[count:first]))
        inner = refs[end + n_out :]
        if late:
            near, sem, inner = inner[: len(late)], inner[len(late)], inner[len(late) + 1 :]
            pairs = enumerate(zip(refs[first:end], near))
            copies = [pltpu.make_async_copy(f, v, sem.at[i]) for i, (f, v) in pairs]
            for copy in copies:
                copy.start()
            given.append(list(zip(near, copies)))
        body(*given, *refs[end : end + n_out], *inner)

    return pl.pallas_call(
        run,
        out_shape=outs,
        in_specs=[pl.BlockSpec(memory_space=s) for s in spaces],
        out_specs=jax.tree.map(lambda _: pl.BlockSpec(memory_space=pltpu.VMEM), outs),
        scratch_shapes=[*held, *scratch],
        cost_estimate=pl.CostEstimate(flops=flops, bytes_accessed=moved, transcendentals=0),
        compiler_params=pltpu.CompilerParams(
            vmem_limit_bytes=(20 if weights or not late else 60) * 1024 * 1024
        ),
    )(*args, *weights, *late)


def dot(a, b):
    return jnp.dot(a, b, preferred_element_type=F32)


def dot_t(a, b):
    return lax.dot_general(a, b, (((1,), (1,)), ((), ())), preferred_element_type=F32)


SPANS = ((0, 512), (512, 512), (1024, 512), (1536, 512))


def block(z, k):
    return pl.ds(pl.multiple_of(lax.rem(z + k, 4) * 512, 512), 512)


def rows_of(index, count):
    return pl.ds(pl.multiple_of(index * count, 16), count)


def times_rows(a, pieces, cols):
    total = None
    for (at, size), p in zip(SPANS, pieces):
        part = dot(a[:, at : at + size], p[:, cols])
        total = part if total is None else total + part
    return total


def copies_kernel(pieces, copies):
    at = 0
    for w, copy in pieces:
        copy.wait()
        part, width = w[...].astype(BF), w.shape[1]
        for y in range(8):
            copies[y, :, at : at + width] = part
        at += width


def copies_scales_kernel(where, value, inner, outer, up, out, down, pieces, copies, line, rows):
    y = where[3]
    f = where[0] * 8 + y
    lane = lax.broadcasted_iota(jnp.int32, (8, 128), 1)
    mix = value[...] * inner[...] * outer[...]
    at = 0
    for v, count, start in ((mix, 2, f * 8), (up[...], 6, f * 24), (out[...], 4, y * 64), (down[...], 4, y * 64)):
        n = v.shape[1]
        line[...] = jnp.zeros((8, 128), F32)
        line[:, 0:n] = jnp.broadcast_to(v, (8, n))
        turned = pltpu.roll(line[...], lax.rem(start, 128), 1)
        for r in range(count):
            place = lane + r * 128
            row = jnp.where((place >= start) & (place < start + n), turned, 0.0)
            rows[at + r : at + r + 1, :] = row[0:1]
        at += count
    left = rows[...]
    for i in range(3):
        part = left.astype(BF)
        left = left - part.astype(F32)
        for k in range(8):
            copies[k, i * 16 : i * 16 + 16, 512:640] = part
    for k in range(8):
        copies[k, 48:64, 512:640] = jnp.zeros((16, 128), BF)
    copies_kernel(pieces, copies)


def read_scales(vi, mix_cols, up_cols, out_cols, down_cols):
    total = None
    for k in range(4):
        parts = vi[k][:, 512:640].astype(F32).reshape(8, 64, 128).sum(axis=0)
        rows = parts[0:16] + parts[16:32] + parts[32:48]
        total = rows if total is None else total + rows
        for i in range(4):
            at = slice(k * 512 + i * 128, k * 512 + i * 128 + 128)
            out_cols[:, at] = rows[8 + i : 9 + i]
            down_cols[:, at] = rows[12 + i : 13 + i]
    for i in range(2):
        mix_cols[:, i * 128 : i * 128 + 128] = total[i : i + 1]
    for i in range(6):
        up_cols[:, i * 128 : i * 128 + 128] = total[2 + i : 3 + i]


def mlp_cast_kernel(pieces, first, second):
    (up, up_copy), (down, down_copy) = pieces
    up_copy.wait()
    first[:, 0:768] = up[...].astype(BF)
    down_copy.wait()
    first[:, 768:1024] = down[:, 0:256].astype(BF)
    second[...] = down[:, 256:768].astype(BF)


def stack_kernel(first, second, third, fourth, stacked):
    for i, w in enumerate((first, second, third, fourth)):
        stacked[i * 64 : i * 64 + 64, :] = w[...]


def norm_kernel(where, tokens, gain, normed, share):
    z, row = where[0], where[1] * 4 + where[2]
    t = tokens[...].astype(F32)
    scale = lax.rsqrt(jnp.mean(t * t, axis=-1, keepdims=True) + norm_eps)
    for k in range(4):
        at = slice(k * 512, k * 512 + 512)
        normed[:, at] = (tokens[:, block(z, k)].astype(F32) * scale * gain[:, block(z, k)]).astype(BF)
        share[:, at] = tokens[rows_of(row, 48), block(z, k)].astype(F32)


def conv_kernel(normed, taps, vi, conv, cols, up_cols, out_cols, down_cols, padded):
    read_scales(vi, cols, up_cols, out_cols, down_cols)
    value = times_rows(normed, vi, slice(0, 256))
    inner = times_rows(normed, vi, slice(256, 512))
    gated = inner * value
    padded[0:8, :] = jnp.zeros((8, 256), F32)
    padded[392:400, :] = jnp.zeros((8, 256), F32)
    padded[8:392, :] = gated
    mixed = taps[0:1, :] * padded[7:391, :] + taps[1:2, :] * gated + taps[2:3, :] * padded[9:393, :]
    conv[...] = mixed * cols[...]


def z_piece(w, k, at, n):
    return w[:, k, :, at : at + n].reshape(512, n)


def hidden_kernel(where, normed, conv, oo, hidden, other):
    outer = times_rows(normed, oo, slice(0, 256))
    hidden[...] = (outer * conv[...]).astype(BF)
    theirs = hidden[rows_of(1 - where[1], 192), :]
    for (at, size), p in zip(SPANS, oo):
        other[:, at : at + size] = dot_t(theirs, p[:, 256:512]).astype(BF)


def mix_kernel(where, hidden, got, oo, mix):
    mine = hidden[rows_of(where[1], 192), :]
    for (at, size), p in zip(SPANS, oo):
        part = dot_t(mine, p[:, 256:512])
        mix[:, at : at + size] = (part + got[:, at : at + size].astype(F32)).astype(BF)


def middle_kernel(where, share, got, cols, gain, middle, copies):
    z = where[0]
    total = got[0].astype(F32) + got[1].astype(F32) + got[2].astype(F32) + got[3].astype(F32)
    mid = share[...] + total * cols[...]
    middle[...] = mid
    scale = lax.rsqrt(jnp.mean(mid * mid, axis=-1, keepdims=True) + norm_eps)
    for k in range(4):
        at = slice(k * 512, k * 512 + 512)
        part = (mid[:, at] * scale * gain[:, block(z, k)]).astype(BF)
        for j in range(4):
            copies[j, :, at] = part


def act_of(rows, ud, cols, act):
    @pl.loop(0, 3)
    def _(i):
        at = pl.ds(pl.multiple_of(i * 256, 256), 256)
        up = times_rows(rows, ud, at) * cols[:, at]
        act[:, at] = jnp.square(jnp.maximum(up, 0.0)).astype(BF)


def up_kernel(rows, cols, ud, act):
    act_of(rows, ud, cols, act)


def down_parts(act, ud, down):
    for k, (at, size) in enumerate(SPANS):
        part = dot_t(act[:, 0:256], ud[k][:, 768:1024])
        yield slice(at, at + size), part + dot_t(act[:, 256:768], z_piece(down, k, 0, 512))


def up_down_kernel(rows, cols, late, other, act):
    for _, copy in late[:4]:
        copy.wait()
    ud = [p for p, _ in late[:4]]
    act_of(rows, ud, cols, act)
    down, copy = late[4]
    copy.wait()
    for at, part in down_parts(act, ud, down):
        other[:, at] = part.astype(BF)


def down_kernel(act, got, pieces, mlp):
    for at, part in down_parts(act, pieces[:4], pieces[4]):
        mlp[:, at] = (part + got[:, at].astype(F32)).astype(BF)


def end_kernel(where, middle, got, cols, copies):
    z = where[0]
    total = got[0].astype(F32) + got[1].astype(F32) + got[2].astype(F32) + got[3].astype(F32)
    end = (middle[...] + total * cols[...]).astype(BF)
    for k in range(4):
        for j in range(4):
            copies[j, :, block(z, k)] = end[:, k * 512 : k * 512 + 512]


def join_kernel(where, mine, theirs, result):
    result[rows_of(where[1], 192), :] = mine[...]
    result[rows_of(1 - where[1], 192), :] = theirs[...]


def body(
    tokens,
    mix_gain,
    value_weight,
    value_scale,
    inner_weight,
    inner_scale,
    outer_weight,
    outer_scale,
    conv_taps,
    out_weight,
    out_scale,
    mlp_gain,
    up_weight,
    up_scale,
    down_weight,
    down_scale,
):
    z = lax.axis_index("zl")
    where = jnp.stack([z, lax.axis_index("c"), lax.axis_index("x"), lax.axis_index("y")]).astype(jnp.int32)

    vi = jnp.concatenate([value_weight.astype(BF), inner_weight.astype(BF)], axis=1)
    small = (value_scale, inner_scale, outer_scale, up_scale, out_scale, down_scale)
    vi = kernel(
        copies_scales_kernel,
        SHAPE((8, 64, 640), BF),
        1_000_000,
        where,
        *[v[None] for v in small],
        late=[value_weight, inner_weight],
        scratch=[pltpu.VMEM((8, 128), F32), pltpu.VMEM((16, 128), F32)],
    )
    vi = spread(vi, "y").reshape(512, 640)
    oo = kernel(
        copies_kernel, SHAPE((8, 64, 512), BF), 1_000_000, late=[outer_weight, out_weight.T]
    )
    oo = spread(oo, "y").reshape(512, 512)
    ud, dn = kernel(
        mlp_cast_kernel,
        (SHAPE((64, 1024), BF), SHAPE((64, 512), BF)),
        1_000_000,
        late=[up_weight, down_weight.T],
    )
    ud = lax.all_gather(ud, "y", axis=0, tiled=True)
    dn = z_then_y(dn, -2)
    normed, share = kernel(
        norm_kernel,
        (SHAPE((384, 2048), BF), SHAPE((48, 2048), F32)),
        10_000_000,
        where,
        tokens[0],
        mix_gain[None],
    )
    vi = along_z(vi, 1)
    oo = along_z(oo, -1)
    ud = along_z(ud, 1)

    wide = SHAPE((1, 2048), F32)
    conv, _, up_cols, out_cols, down_cols = kernel(
        conv_kernel,
        (SHAPE((384, 256), F32), SHAPE((1, 256), F32), SHAPE((1, 768), F32), wide, wide),
        800_000_000,
        normed,
        conv_taps,
        weights=vi,
        scratch=[pltpu.VMEM((400, 256), F32)],
    )
    hidden, mix_other = kernel(
        hidden_kernel,
        (SHAPE((384, 256), BF), SHAPE((192, 2048), BF)),
        600_000_000,
        where,
        normed,
        conv,
        weights=oo,
    )
    got = swap_cores(mix_other)
    mix = kernel(mix_kernel, SHAPE((192, 2048), BF), 200_000_000, where, hidden, got, weights=oo)
    mix = spread(mix.reshape(4, 48, 2048), "x")
    middle, copies = kernel(
        middle_kernel,
        (SHAPE((48, 2048), F32), SHAPE((4, 48, 2048), BF)),
        2_000_000,
        where,
        share,
        mix,
        out_cols,
        mlp_gain[None],
    )
    own = spread(copies, "x").reshape(192, 2048)
    other = swap_cores(own)
    act = kernel(up_kernel, SHAPE((192, 768), BF), 600_000_000, own, up_cols, weights=ud)
    mlp_other = kernel(
        up_down_kernel,
        SHAPE((192, 2048), BF),
        1_200_000_000,
        other,
        up_cols,
        late=[*ud, dn],
        scratch=[pltpu.VMEM((192, 768), BF)],
    )
    got = swap_cores(mlp_other)
    mlp = kernel(down_kernel, SHAPE((192, 2048), BF), 600_000_000, act, got, weights=[*ud, dn])
    mlp = spread(mlp.reshape(4, 48, 2048), "x")
    copies = kernel(end_kernel, SHAPE((4, 48, 2048), BF), 2_000_000, where, middle, mlp, down_cols)
    mine = spread(copies, "x").reshape(192, 2048)
    theirs = swap_cores(mine)
    result = kernel(join_kernel, SHAPE((384, 2048), BF), 1_000_000, where, mine, theirs)
    return result[None]


def solution(mesh):
    fine = Mesh(mesh.devices.reshape(2, 4, 8, 4, 2), ("zh", "zl", "y", "x", "c"))
    rows = P(("zh", "zl", "y"), None, None)
    fs, tp = ("zl", "y"), ("x", "c")
    all_cols = P(tp + fs)
    placed = (
        rows,
        P(),
        P(fs, tp),
        all_cols,
        P(fs, tp),
        all_cols,
        P(fs, tp),
        all_cols,
        P(None, tp),
        P(tp, fs),
        P(fs),
        P(),
        P(fs, tp),
        all_cols,
        P(tp, fs),
        P(fs),
    )
    return jax.shard_map(body, mesh=fine, in_specs=placed, out_specs=rows, check_vma=False)
```

```python
import jax
import jax.numpy as jnp
from jax import lax
from jax.experimental import pallas as pl
from jax.experimental.pallas import tpu as pltpu
from jax.sharding import Mesh, PartitionSpec as P


norm_eps = 1e-06

Z = ("zh", "zl")
BF = jnp.bfloat16
F32 = jnp.float32
SHAPE = jax.ShapeDtypeStruct


def z_shift(a, step):
    return lax.ppermute(a, Z, [(i, (i + step) % 8) for i in range(8)])


def swap_cores(a):
    return lax.ppermute(a, "c", [(0, 1), (1, 0)])


def spread(a, axis):
    return lax.all_to_all(a, axis, 0, 0, tiled=True)


def along_z(got, far):
    before = z_shift(got, 1)
    after = z_shift(got, -1)
    return [got, after, z_shift(before if far > 0 else after, far), before]


def z_then_y(a, far):
    near = [z_shift(a, step) for step in (-1, far, 1)]
    width = a.shape[1]
    stacked = kernel(stack_kernel, SHAPE((256, width), BF), 1_000_000, a, *near)
    return lax.all_gather(stacked, "y", axis=0, tiled=True).reshape(8, 4, 64, width)


def kernel(body, outs, flops, *args, weights=(), late=(), scratch=()):
    spaces = [pltpu.SMEM if a.dtype == jnp.int32 else pltpu.VMEM for a in (*args, *weights)]
    spaces += [pl.ANY] * len(late)
    moved = sum(a.size * a.dtype.itemsize for a in (*args, *weights, *late))
    held = [pltpu.VMEM(w.shape, w.dtype) for w in late]
    held += [pltpu.SemaphoreType.DMA((len(late),))] if late else []
    count, n_out = len(args), len(jax.tree.leaves(outs))

    def run(*refs):
        given, first, end = list(refs[:count]), count + len(weights), count + len(weights) + len(late)
        if weights:
            given.append(list(refs[count:first]))
        inner = refs[end + n_out :]
        if late:
            near, sem, inner = inner[: len(late)], inner[len(late)], inner[len(late) + 1 :]
            pairs = enumerate(zip(refs[first:end], near))
            copies = [pltpu.make_async_copy(f, v, sem.at[i]) for i, (f, v) in pairs]
            for copy in copies:
                copy.start()
            given.append(list(zip(near, copies)))
        body(*given, *refs[end : end + n_out], *inner)

    return pl.pallas_call(
        run,
        out_shape=outs,
        in_specs=[pl.BlockSpec(memory_space=s) for s in spaces],
        out_specs=jax.tree.map(lambda _: pl.BlockSpec(memory_space=pltpu.VMEM), outs),
        scratch_shapes=[*held, *scratch],
        cost_estimate=pl.CostEstimate(flops=flops, bytes_accessed=moved, transcendentals=0),
        compiler_params=pltpu.CompilerParams(
            vmem_limit_bytes=(20 if weights or not late else 60) * 1024 * 1024
        ),
    )(*args, *weights, *late)


def dot(a, b):
    return jnp.dot(a, b, preferred_element_type=F32)


def dot_t(a, b):
    return lax.dot_general(a, b, (((1,), (1,)), ((), ())), preferred_element_type=F32)


SPANS = ((0, 512), (512, 512), (1024, 512), (1536, 512))


def block(z, k):
    return pl.ds(pl.multiple_of(lax.rem(z + k, 4) * 512, 512), 512)


def rows_of(index, count):
    return pl.ds(pl.multiple_of(index * count, 16), count)


def times_rows(a, pieces, cols):
    total = None
    for (at, size), p in zip(SPANS, pieces):
        part = dot(a[:, at : at + size], p[:, cols])
        total = part if total is None else total + part
    return total


def copies_kernel(pieces, copies):
    at = 0
    for w, copy in pieces:
        copy.wait()
        part, width = w[...].astype(BF), w.shape[1]
        for y in range(8):
            copies[y, :, at : at + width] = part
        at += width


def copies_scales_kernel(where, value, inner, outer, up, out, down, pieces, copies, line, rows):
    y = where[3]
    f = where[0] * 8 + y
    lane = lax.broadcasted_iota(jnp.int32, (8, 128), 1)
    mix = value[...] * inner[...] * outer[...]
    at = 0
    for v, count, start in ((mix, 2, f * 8), (up[...], 6, f * 24), (out[...], 4, y * 64), (down[...], 4, y * 64)):
        n = v.shape[1]
        line[...] = jnp.zeros((8, 128), F32)
        line[:, 0:n] = jnp.broadcast_to(v, (8, n))
        turned = pltpu.roll(line[...], lax.rem(start, 128), 1)
        for r in range(count):
            place = lane + r * 128
            row = jnp.where((place >= start) & (place < start + n), turned, 0.0)
            rows[at + r : at + r + 1, :] = row[0:1]
        at += count
    left = rows[...]
    for i in range(3):
        part = left.astype(BF)
        left = left - part.astype(F32)
        for k in range(8):
            copies[k, i * 16 : i * 16 + 16, 512:640] = part
    for k in range(8):
        copies[k, 48:64, 512:640] = jnp.zeros((16, 128), BF)
    copies_kernel(pieces, copies)


def read_scales(vi, mix_cols, up_cols, out_cols, down_cols):
    total = None
    for k in range(4):
        parts = vi[k][:, 512:640].astype(F32).reshape(8, 64, 128).sum(axis=0)
        rows = parts[0:16] + parts[16:32] + parts[32:48]
        total = rows if total is None else total + rows
        for i in range(4):
            at = slice(k * 512 + i * 128, k * 512 + i * 128 + 128)
            out_cols[:, at] = rows[8 + i : 9 + i]
            down_cols[:, at] = rows[12 + i : 13 + i]
    for i in range(2):
        mix_cols[:, i * 128 : i * 128 + 128] = total[i : i + 1]
    for i in range(6):
        up_cols[:, i * 128 : i * 128 + 128] = total[2 + i : 3 + i]


def mlp_cast_kernel(pieces, up, down):
    copies_kernel(pieces[:1], up)
    w, copy = pieces[1]
    copy.wait()
    down[...] = w[...].astype(BF)


def side_kernel(pieces, both):
    at = 0
    for w, copy in pieces:
        copy.wait()
        both[:, at : at + w.shape[1]] = w[...].astype(BF)
        at += w.shape[1]


def stack_kernel(first, second, third, fourth, stacked):
    for i, w in enumerate((first, second, third, fourth)):
        stacked[i * 64 : i * 64 + 64, :] = w[...]


def norm_kernel(where, tokens, gain, normed, share):
    z, row = where[0], where[1] * 4 + where[2]
    t = tokens[...].astype(F32)
    scale = lax.rsqrt(jnp.mean(t * t, axis=-1, keepdims=True) + norm_eps)
    for k in range(4):
        at = slice(k * 512, k * 512 + 512)
        normed[:, at] = (tokens[:, block(z, k)].astype(F32) * scale * gain[:, block(z, k)]).astype(BF)
        share[:, at] = tokens[rows_of(row, 48), block(z, k)].astype(F32)


def conv_kernel(normed, taps, vi, conv, cols, up_cols, out_cols, down_cols, padded):
    read_scales(vi, cols, up_cols, out_cols, down_cols)
    value = times_rows(normed, vi, slice(0, 256))
    inner = times_rows(normed, vi, slice(256, 512))
    gated = inner * value
    padded[0:8, :] = jnp.zeros((8, 256), F32)
    padded[392:400, :] = jnp.zeros((8, 256), F32)
    padded[8:392, :] = gated
    mixed = taps[0:1, :] * padded[7:391, :] + taps[1:2, :] * gated + taps[2:3, :] * padded[9:393, :]
    conv[...] = mixed * cols[...]


def z_piece(w, k, at, n):
    return w[:, k, :, at : at + n].reshape(512, n)


def hidden_kernel(where, normed, conv, oo, hidden, other):
    outer = times_rows(normed, [z_piece(oo[0], k, 0, 256) for k in range(4)], slice(0, 256))
    hidden[...] = (outer * conv[...]).astype(BF)
    theirs = hidden[rows_of(1 - where[1], 192), :]
    for k, (at, size) in enumerate(SPANS):
        other[:, at : at + size] = dot_t(theirs, z_piece(oo[0], k, 256, 256)).astype(BF)


def mix_kernel(where, hidden, got, oo, mix):
    mine = hidden[rows_of(where[1], 192), :]
    for k, (at, size) in enumerate(SPANS):
        part = dot_t(mine, z_piece(oo[0], k, 256, 256))
        mix[:, at : at + size] = (part + got[:, at : at + size].astype(F32)).astype(BF)


def middle_kernel(where, share, got, cols, gain, middle, copies):
    z = where[0]
    total = got[0].astype(F32) + got[1].astype(F32) + got[2].astype(F32) + got[3].astype(F32)
    mid = share[...] + total * cols[...]
    middle[...] = mid
    scale = lax.rsqrt(jnp.mean(mid * mid, axis=-1, keepdims=True) + norm_eps)
    for k in range(4):
        at = slice(k * 512, k * 512 + 512)
        part = (mid[:, at] * scale * gain[:, block(z, k)]).astype(BF)
        for j in range(4):
            copies[j, :, at] = part


def act_of(rows, ud, cols, act):
    @pl.loop(0, 3)
    def _(i):
        at = pl.ds(pl.multiple_of(i * 256, 256), 256)
        up = times_rows(rows, ud, at) * cols[:, at]
        act[:, at] = jnp.square(jnp.maximum(up, 0.0)).astype(BF)


def up_kernel(rows, cols, ud, act):
    act_of(rows, ud, cols, act)


def down_parts(act, down):
    for k, (at, size) in enumerate(SPANS):
        yield slice(at, at + size), dot_t(act[...], z_piece(down, k, 0, 768))


def up_down_kernel(rows, cols, late, other, act):
    for _, copy in late[:4]:
        copy.wait()
    act_of(rows, [p for p, _ in late[:4]], cols, act)
    down, copy = late[4]
    copy.wait()
    for at, part in down_parts(act, down):
        other[:, at] = part.astype(BF)


def down_kernel(act, got, pieces, mlp):
    for at, part in down_parts(act, pieces[0]):
        mlp[:, at] = (part + got[:, at].astype(F32)).astype(BF)


def end_kernel(where, middle, got, cols, copies):
    z = where[0]
    total = got[0].astype(F32) + got[1].astype(F32) + got[2].astype(F32) + got[3].astype(F32)
    end = (middle[...] + total * cols[...]).astype(BF)
    for k in range(4):
        for j in range(4):
            copies[j, :, block(z, k)] = end[:, k * 512 : k * 512 + 512]


def join_kernel(where, mine, theirs, result):
    result[rows_of(where[1], 192), :] = mine[...]
    result[rows_of(1 - where[1], 192), :] = theirs[...]


def body(
    tokens,
    mix_gain,
    value_weight,
    value_scale,
    inner_weight,
    inner_scale,
    outer_weight,
    outer_scale,
    conv_taps,
    out_weight,
    out_scale,
    mlp_gain,
    up_weight,
    up_scale,
    down_weight,
    down_scale,
):
    z = lax.axis_index("zl")
    where = jnp.stack([z, lax.axis_index("c"), lax.axis_index("x"), lax.axis_index("y")]).astype(jnp.int32)

    vi = jnp.concatenate([value_weight.astype(BF), inner_weight.astype(BF)], axis=1)
    small = (value_scale, inner_scale, outer_scale, up_scale, out_scale, down_scale)
    vi = kernel(
        copies_scales_kernel,
        SHAPE((8, 64, 640), BF),
        1_000_000,
        where,
        *[v[None] for v in small],
        late=[value_weight, inner_weight],
        scratch=[pltpu.VMEM((8, 128), F32), pltpu.VMEM((16, 128), F32)],
    )
    vi = spread(vi, "y").reshape(512, 640)
    oo = kernel(side_kernel, SHAPE((64, 512), BF), 1_000_000, late=[outer_weight, out_weight.T])
    up, dn = kernel(
        mlp_cast_kernel,
        (SHAPE((8, 64, 768), BF), SHAPE((64, 768), BF)),
        1_000_000,
        late=[up_weight, down_weight.T],
    )
    oo = z_then_y(oo, 2)
    up = spread(up, "y").reshape(512, 768)
    dn = z_then_y(dn, -2)
    normed, share = kernel(
        norm_kernel,
        (SHAPE((384, 2048), BF), SHAPE((48, 2048), F32)),
        10_000_000,
        where,
        tokens[0],
        mix_gain[None],
    )
    vi = along_z(vi, 1)
    up = along_z(up, 1)

    wide = SHAPE((1, 2048), F32)
    conv, _, up_cols, out_cols, down_cols = kernel(
        conv_kernel,
        (SHAPE((384, 256), F32), SHAPE((1, 256), F32), SHAPE((1, 768), F32), wide, wide),
        800_000_000,
        normed,
        conv_taps,
        weights=vi,
        scratch=[pltpu.VMEM((400, 256), F32)],
    )
    hidden, mix_other = kernel(
        hidden_kernel,
        (SHAPE((384, 256), BF), SHAPE((192, 2048), BF)),
        600_000_000,
        where,
        normed,
        conv,
        weights=[oo],
    )
    got = swap_cores(mix_other)
    mix = kernel(mix_kernel, SHAPE((192, 2048), BF), 200_000_000, where, hidden, got, weights=[oo])
    mix = spread(mix.reshape(4, 48, 2048), "x")
    middle, copies = kernel(
        middle_kernel,
        (SHAPE((48, 2048), F32), SHAPE((4, 48, 2048), BF)),
        2_000_000,
        where,
        share,
        mix,
        out_cols,
        mlp_gain[None],
    )
    own = spread(copies, "x").reshape(192, 2048)
    other = swap_cores(own)
    act = kernel(up_kernel, SHAPE((192, 768), BF), 600_000_000, own, up_cols, weights=up)
    mlp_other = kernel(
        up_down_kernel,
        SHAPE((192, 2048), BF),
        1_200_000_000,
        other,
        up_cols,
        late=[*up, dn],
        scratch=[pltpu.VMEM((192, 768), BF)],
    )
    got = swap_cores(mlp_other)
    mlp = kernel(down_kernel, SHAPE((192, 2048), BF), 600_000_000, act, got, weights=[dn])
    mlp = spread(mlp.reshape(4, 48, 2048), "x")
    copies = kernel(end_kernel, SHAPE((4, 48, 2048), BF), 2_000_000, where, middle, mlp, down_cols)
    mine = spread(copies, "x").reshape(192, 2048)
    theirs = swap_cores(mine)
    result = kernel(join_kernel, SHAPE((384, 2048), BF), 1_000_000, where, mine, theirs)
    return result[None]


def solution(mesh):
    fine = Mesh(mesh.devices.reshape(2, 4, 8, 4, 2), ("zh", "zl", "y", "x", "c"))
    rows = P(("zh", "zl", "y"), None, None)
    fs, tp = ("zl", "y"), ("x", "c")
    all_cols = P(tp + fs)
    placed = (
        rows,
        P(),
        P(fs, tp),
        all_cols,
        P(fs, tp),
        all_cols,
        P(fs, tp),
        all_cols,
        P(None, tp),
        P(tp, fs),
        P(fs),
        P(),
        P(fs, tp),
        all_cols,
        P(tp, fs),
        P(fs),
    )
    return jax.shard_map(body, mesh=fine, in_specs=placed, out_specs=rows, check_vma=False)
```

```python
import jax
import jax.numpy as jnp
from jax import lax
from jax.experimental import pallas as pl
from jax.experimental.pallas import tpu as pltpu
from jax.sharding import Mesh, PartitionSpec as P


norm_eps = 1e-06

Z = ("zh", "zl")
BF = jnp.bfloat16
F32 = jnp.float32
SHAPE = jax.ShapeDtypeStruct


def z_shift(a, step):
    return lax.ppermute(a, Z, [(i, (i + step) % 8) for i in range(8)])


def swap_cores(a):
    return lax.ppermute(a, "c", [(0, 1), (1, 0)])


def spread(a, axis):
    return lax.all_to_all(a, axis, 0, 0, tiled=True)


def along_z(got, far):
    before = z_shift(got, 1)
    after = z_shift(got, -1)
    return [got, after, z_shift(before if far > 0 else after, far), before]


def z_then_y(a, far):
    near = [z_shift(a, step) for step in (-1, far, 1)]
    width = a.shape[1]
    stacked = kernel(stack_kernel, SHAPE((256, width), BF), 1_000_000, a, *near)
    return lax.all_gather(stacked, "y", axis=0, tiled=True).reshape(8, 4, 64, width)


def kernel(body, outs, flops, *args, weights=(), late=(), scratch=()):
    spaces = [pltpu.SMEM if a.dtype == jnp.int32 else pltpu.VMEM for a in (*args, *weights)]
    spaces += [pl.ANY] * len(late)
    moved = sum(a.size * a.dtype.itemsize for a in (*args, *weights, *late))
    held = [pltpu.VMEM(w.shape, w.dtype) for w in late]
    held += [pltpu.SemaphoreType.DMA((len(late),))] if late else []
    count, n_out = len(args), len(jax.tree.leaves(outs))

    def run(*refs):
        given, first, end = list(refs[:count]), count + len(weights), count + len(weights) + len(late)
        if weights:
            given.append(list(refs[count:first]))
        inner = refs[end + n_out :]
        if late:
            near, sem, inner = inner[: len(late)], inner[len(late)], inner[len(late) + 1 :]
            pairs = enumerate(zip(refs[first:end], near))
            copies = [pltpu.make_async_copy(f, v, sem.at[i]) for i, (f, v) in pairs]
            for copy in copies:
                copy.start()
            given.append(list(zip(near, copies)))
        body(*given, *refs[end : end + n_out], *inner)

    return pl.pallas_call(
        run,
        out_shape=outs,
        in_specs=[pl.BlockSpec(memory_space=s) for s in spaces],
        out_specs=jax.tree.map(lambda _: pl.BlockSpec(memory_space=pltpu.VMEM), outs),
        scratch_shapes=[*held, *scratch],
        cost_estimate=pl.CostEstimate(flops=flops, bytes_accessed=moved, transcendentals=0),
        compiler_params=pltpu.CompilerParams(
            vmem_limit_bytes=(20 if weights or not late else 60) * 1024 * 1024
        ),
    )(*args, *weights, *late)


def dot(a, b):
    return jnp.dot(a, b, preferred_element_type=F32)


def dot_t(a, b):
    return lax.dot_general(a, b, (((1,), (1,)), ((), ())), preferred_element_type=F32)


SPANS = ((0, 512), (512, 512), (1024, 512), (1536, 512))


def block(z, k):
    return pl.ds(pl.multiple_of(lax.rem(z + k, 4) * 512, 512), 512)


def rows_of(index, count):
    return pl.ds(pl.multiple_of(index * count, 16), count)


def times_rows(a, pieces, cols):
    total = None
    for (at, size), p in zip(SPANS, pieces):
        part = dot(a[:, at : at + size], p[:, cols])
        total = part if total is None else total + part
    return total


def copies_kernel(pieces, copies):
    at = 0
    for w, copy in pieces:
        copy.wait()
        part, width = w[...].astype(BF), w.shape[1]
        for y in range(8):
            copies[y, :, at : at + width] = part
        at += width


def copies_scales_kernel(where, value, inner, outer, up, out, down, pieces, copies, line, rows):
    y = where[3]
    f = where[0] * 8 + y
    lane = lax.broadcasted_iota(jnp.int32, (8, 128), 1)
    mix = value[...] * inner[...] * outer[...]
    at = 0
    for v, count, start in ((mix, 2, f * 8), (up[...], 6, f * 24), (out[...], 4, y * 64), (down[...], 4, y * 64)):
        n = v.shape[1]
        line[...] = jnp.zeros((8, 128), F32)
        line[:, 0:n] = jnp.broadcast_to(v, (8, n))
        turned = pltpu.roll(line[...], lax.rem(start, 128), 1)
        for r in range(count):
            place = lane + r * 128
            row = jnp.where((place >= start) & (place < start + n), turned, 0.0)
            rows[at + r : at + r + 1, :] = row[0:1]
        at += count
    left = rows[...]
    for i in range(3):
        part = left.astype(BF)
        left = left - part.astype(F32)
        for k in range(8):
            copies[k, i * 16 : i * 16 + 16, 512:640] = part
    for k in range(8):
        copies[k, 48:64, 512:640] = jnp.zeros((16, 128), BF)
    copies_kernel(pieces, copies)


def read_scales(vi, mix_cols, up_cols, out_cols, down_cols):
    total = None
    for k in range(4):
        parts = vi[k][:, 512:640].astype(F32).reshape(8, 64, 128).sum(axis=0)
        rows = parts[0:16] + parts[16:32] + parts[32:48]
        total = rows if total is None else total + rows
        for i in range(4):
            at = slice(k * 512 + i * 128, k * 512 + i * 128 + 128)
            out_cols[:, at] = rows[8 + i : 9 + i]
            down_cols[:, at] = rows[12 + i : 13 + i]
    for i in range(2):
        mix_cols[:, i * 128 : i * 128 + 128] = total[i : i + 1]
    for i in range(6):
        up_cols[:, i * 128 : i * 128 + 128] = total[2 + i : 3 + i]


def mlp_cast_kernel(pieces, up, down):
    copies_kernel(pieces[:1], up)
    w, copy = pieces[1]
    copy.wait()
    down[...] = w[...].astype(BF)


def side_kernel(pieces, both):
    at = 0
    for w, copy in pieces:
        copy.wait()
        both[:, at : at + w.shape[1]] = w[...].astype(BF)
        at += w.shape[1]


def stack_kernel(first, second, third, fourth, stacked):
    for i, w in enumerate((first, second, third, fourth)):
        stacked[i * 64 : i * 64 + 64, :] = w[...]


def norm_kernel(where, tokens, gain, normed, share):
    z, row = where[0], where[1] * 4 + where[2]
    t = tokens[...].astype(F32)
    scale = lax.rsqrt(jnp.mean(t * t, axis=-1, keepdims=True) + norm_eps)
    for k in range(4):
        at = slice(k * 512, k * 512 + 512)
        normed[:, at] = (tokens[:, block(z, k)].astype(F32) * scale * gain[:, block(z, k)]).astype(BF)
        share[:, at] = tokens[rows_of(row, 48), block(z, k)].astype(F32)


def conv_kernel(normed, taps, vi, conv, cols, up_cols, out_cols, down_cols, padded):
    read_scales(vi, cols, up_cols, out_cols, down_cols)
    value = times_rows(normed, vi, slice(0, 256))
    inner = times_rows(normed, vi, slice(256, 512))
    gated = inner * value
    padded[0:8, :] = jnp.zeros((8, 256), F32)
    padded[392:400, :] = jnp.zeros((8, 256), F32)
    padded[8:392, :] = gated
    mixed = taps[0:1, :] * padded[7:391, :] + taps[1:2, :] * gated + taps[2:3, :] * padded[9:393, :]
    conv[...] = mixed * cols[...]


def z_piece(w, k, at, n):
    return w[:, k, :, at : at + n].reshape(512, n)


def hidden_kernel(where, normed, conv, oo, hidden, other):
    outer = times_rows(normed, [z_piece(oo[0], k, 0, 256) for k in range(4)], slice(0, 256))
    hidden[...] = (outer * conv[...]).astype(BF)
    theirs = hidden[rows_of(1 - where[1], 192), :]
    for k, (at, size) in enumerate(SPANS):
        other[:, at : at + size] = dot_t(theirs, z_piece(oo[0], k, 256, 256)).astype(BF)


def mix_kernel(where, hidden, got, oo, mix):
    mine = hidden[rows_of(where[1], 192), :]
    for k, (at, size) in enumerate(SPANS):
        part = dot_t(mine, z_piece(oo[0], k, 256, 256))
        mix[:, at : at + size] = (part + got[:, at : at + size].astype(F32)).astype(BF)


def middle_kernel(where, share, got, cols, gain, middle, copies):
    z = where[0]
    total = got[0].astype(F32) + got[1].astype(F32) + got[2].astype(F32) + got[3].astype(F32)
    mid = share[...] + total * cols[...]
    middle[...] = mid
    scale = lax.rsqrt(jnp.mean(mid * mid, axis=-1, keepdims=True) + norm_eps)
    for k in range(4):
        at = slice(k * 512, k * 512 + 512)
        part = (mid[:, at] * scale * gain[:, block(z, k)]).astype(BF)
        for j in range(4):
            copies[j, :, at] = part


def act_of(rows, ud, cols, act):
    @pl.loop(0, 3)
    def _(i):
        at = pl.ds(pl.multiple_of(i * 256, 256), 256)
        up = times_rows(rows, ud, at) * cols[:, at]
        act[:, at] = jnp.square(jnp.maximum(up, 0.0)).astype(BF)


def up_kernel(rows, cols, ud, act):
    act_of(rows, ud, cols, act)


def down_parts(act, down):
    for k, (at, size) in enumerate(SPANS):
        yield slice(at, at + size), dot_t(act[...], z_piece(down, k, 0, 768))


def up_down_kernel(rows, cols, late, other, act, total):
    for k, ((at, size), (p, copy)) in enumerate(zip(SPANS, late)):
        copy.wait()
        for n in range(0, 768, 256):
            part = dot(rows[:, at : at + size], p[:, n : n + 256])
            if k:
                part = part + total[:, n : n + 256]
            if k < 3:
                total[:, n : n + 256] = part
            else:
                up = part * cols[:, n : n + 256]
                act[:, n : n + 256] = jnp.square(jnp.maximum(up, 0.0)).astype(BF)
    down, copy = late[4]
    copy.wait()
    for at, part in down_parts(act, down):
        other[:, at] = part.astype(BF)


def down_kernel(act, got, pieces, mlp):
    for at, part in down_parts(act, pieces[0]):
        mlp[:, at] = (part + got[:, at].astype(F32)).astype(BF)


def end_kernel(where, middle, got, cols, copies):
    z = where[0]
    total = got[0].astype(F32) + got[1].astype(F32) + got[2].astype(F32) + got[3].astype(F32)
    end = (middle[...] + total * cols[...]).astype(BF)
    for k in range(4):
        for j in range(4):
            copies[j, :, block(z, k)] = end[:, k * 512 : k * 512 + 512]


def join_kernel(where, mine, theirs, result):
    result[rows_of(where[1], 192), :] = mine[...]
    result[rows_of(1 - where[1], 192), :] = theirs[...]


def body(
    tokens,
    mix_gain,
    value_weight,
    value_scale,
    inner_weight,
    inner_scale,
    outer_weight,
    outer_scale,
    conv_taps,
    out_weight,
    out_scale,
    mlp_gain,
    up_weight,
    up_scale,
    down_weight,
    down_scale,
):
    z = lax.axis_index("zl")
    where = jnp.stack([z, lax.axis_index("c"), lax.axis_index("x"), lax.axis_index("y")]).astype(jnp.int32)

    vi = jnp.concatenate([value_weight.astype(BF), inner_weight.astype(BF)], axis=1)
    small = (value_scale, inner_scale, outer_scale, up_scale, out_scale, down_scale)
    vi = kernel(
        copies_scales_kernel,
        SHAPE((8, 64, 640), BF),
        1_000_000,
        where,
        *[v[None] for v in small],
        late=[value_weight, inner_weight],
        scratch=[pltpu.VMEM((8, 128), F32), pltpu.VMEM((16, 128), F32)],
    )
    vi = spread(vi, "y").reshape(512, 640)
    oo = kernel(side_kernel, SHAPE((64, 512), BF), 1_000_000, late=[outer_weight, out_weight.T])
    up, dn = kernel(
        mlp_cast_kernel,
        (SHAPE((8, 64, 768), BF), SHAPE((64, 768), BF)),
        1_000_000,
        late=[up_weight, down_weight.T],
    )
    oo = z_then_y(oo, 2)
    up = spread(up, "y").reshape(512, 768)
    dn = z_then_y(dn, -2)
    normed, share = kernel(
        norm_kernel,
        (SHAPE((384, 2048), BF), SHAPE((48, 2048), F32)),
        10_000_000,
        where,
        tokens[0],
        mix_gain[None],
    )
    vi = along_z(vi, 1)
    up = along_z(up, 1)

    wide = SHAPE((1, 2048), F32)
    conv, _, up_cols, out_cols, down_cols = kernel(
        conv_kernel,
        (SHAPE((384, 256), F32), SHAPE((1, 256), F32), SHAPE((1, 768), F32), wide, wide),
        800_000_000,
        normed,
        conv_taps,
        weights=vi,
        scratch=[pltpu.VMEM((400, 256), F32)],
    )
    hidden, mix_other = kernel(
        hidden_kernel,
        (SHAPE((384, 256), BF), SHAPE((192, 2048), BF)),
        600_000_000,
        where,
        normed,
        conv,
        weights=[oo],
    )
    got = swap_cores(mix_other)
    mix = kernel(mix_kernel, SHAPE((192, 2048), BF), 200_000_000, where, hidden, got, weights=[oo])
    mix = spread(mix.reshape(4, 48, 2048), "x")
    middle, copies = kernel(
        middle_kernel,
        (SHAPE((48, 2048), F32), SHAPE((4, 48, 2048), BF)),
        2_000_000,
        where,
        share,
        mix,
        out_cols,
        mlp_gain[None],
    )
    own = spread(copies, "x").reshape(192, 2048)
    other = swap_cores(own)
    act = kernel(up_kernel, SHAPE((192, 768), BF), 600_000_000, own, up_cols, weights=up)
    mlp_other = kernel(
        up_down_kernel,
        SHAPE((192, 2048), BF),
        1_200_000_000,
        other,
        up_cols,
        late=[*up, dn],
        scratch=[pltpu.VMEM((192, 768), BF), pltpu.VMEM((192, 768), F32)],
    )
    got = swap_cores(mlp_other)
    mlp = kernel(down_kernel, SHAPE((192, 2048), BF), 600_000_000, act, got, weights=[dn])
    mlp = spread(mlp.reshape(4, 48, 2048), "x")
    copies = kernel(end_kernel, SHAPE((4, 48, 2048), BF), 2_000_000, where, middle, mlp, down_cols)
    mine = spread(copies, "x").reshape(192, 2048)
    theirs = swap_cores(mine)
    result = kernel(join_kernel, SHAPE((384, 2048), BF), 1_000_000, where, mine, theirs)
    return result[None]


def solution(mesh):
    fine = Mesh(mesh.devices.reshape(2, 4, 8, 4, 2), ("zh", "zl", "y", "x", "c"))
    rows = P(("zh", "zl", "y"), None, None)
    fs, tp = ("zl", "y"), ("x", "c")
    all_cols = P(tp + fs)
    placed = (
        rows,
        P(),
        P(fs, tp),
        all_cols,
        P(fs, tp),
        all_cols,
        P(fs, tp),
        all_cols,
        P(None, tp),
        P(tp, fs),
        P(fs),
        P(),
        P(fs, tp),
        all_cols,
        P(tp, fs),
        P(fs),
    )
    return jax.shard_map(body, mesh=fine, in_specs=placed, out_specs=rows, check_vma=False)
```

```python
import jax
import jax.numpy as jnp
from jax import lax
from jax.experimental import pallas as pl
from jax.experimental.pallas import tpu as pltpu
from jax.sharding import Mesh, PartitionSpec as P


norm_eps = 1e-06

Z = ("zh", "zl")
BF = jnp.bfloat16
F32 = jnp.float32
SHAPE = jax.ShapeDtypeStruct


def z_shift(a, step):
    return lax.ppermute(a, Z, [(i, (i + step) % 8) for i in range(8)])


def swap_cores(a):
    return lax.ppermute(a, "c", [(0, 1), (1, 0)])


def spread(a, axis):
    return lax.all_to_all(a, axis, 0, 0, tiled=True)


def along_z(got, far):
    before = z_shift(got, 1)
    after = z_shift(got, -1)
    return [got, after, z_shift(before if far > 0 else after, far), before]


def z_then_y(a, far):
    near = [z_shift(a, step) for step in (-1, far, 1)]
    width = a.shape[1]
    stacked = kernel(stack_kernel, SHAPE((256, width), BF), 1_000_000, a, *near)
    return lax.all_gather(stacked, "y", axis=0, tiled=True).reshape(8, 4, 64, width)


def kernel(body, outs, flops, *args, weights=(), late=(), scratch=()):
    spaces = [pltpu.SMEM if a.dtype == jnp.int32 else pltpu.VMEM for a in (*args, *weights)]
    spaces += [pl.ANY] * len(late)
    moved = sum(a.size * a.dtype.itemsize for a in (*args, *weights, *late))
    held = [pltpu.VMEM(w.shape, w.dtype) for w in late]
    held += [pltpu.SemaphoreType.DMA((len(late),))] if late else []
    count, n_out = len(args), len(jax.tree.leaves(outs))

    def run(*refs):
        given, first, end = list(refs[:count]), count + len(weights), count + len(weights) + len(late)
        if weights:
            given.append(list(refs[count:first]))
        inner = refs[end + n_out :]
        if late:
            near, sem, inner = inner[: len(late)], inner[len(late)], inner[len(late) + 1 :]
            pairs = enumerate(zip(refs[first:end], near))
            copies = [pltpu.make_async_copy(f, v, sem.at[i]) for i, (f, v) in pairs]
            for copy in copies:
                copy.start()
            given.append(list(zip(near, copies)))
        body(*given, *refs[end : end + n_out], *inner)

    return pl.pallas_call(
        run,
        out_shape=outs,
        in_specs=[pl.BlockSpec(memory_space=s) for s in spaces],
        out_specs=jax.tree.map(lambda _: pl.BlockSpec(memory_space=pltpu.VMEM), outs),
        scratch_shapes=[*held, *scratch],
        cost_estimate=pl.CostEstimate(flops=flops, bytes_accessed=moved, transcendentals=0),
        compiler_params=pltpu.CompilerParams(
            vmem_limit_bytes=(20 if weights or not late else 60) * 1024 * 1024
        ),
    )(*args, *weights, *late)


def dot(a, b):
    return jnp.dot(a, b, preferred_element_type=F32)


def dot_t(a, b):
    return lax.dot_general(a, b, (((1,), (1,)), ((), ())), preferred_element_type=F32)


SPANS = ((0, 512), (512, 512), (1024, 512), (1536, 512))


def block(z, k):
    return pl.ds(pl.multiple_of(lax.rem(z + k, 4) * 512, 512), 512)


def rows_of(index, count):
    return pl.ds(pl.multiple_of(index * count, 16), count)


def times_rows(a, pieces, cols):
    total = None
    for (at, size), p in zip(SPANS, pieces):
        part = dot(a[:, at : at + size], p[:, cols])
        total = part if total is None else total + part
    return total


def copies_kernel(pieces, copies):
    at = 0
    for w, copy in pieces:
        copy.wait()
        part, width = w[...].astype(BF), w.shape[1]
        for y in range(8):
            copies[y, :, at : at + width] = part
        at += width


def copies_scales_kernel(where, value, inner, outer, up, out, down, pieces, copies, line, rows):
    y = where[3]
    f = where[0] * 8 + y
    lane = lax.broadcasted_iota(jnp.int32, (8, 128), 1)
    mix = value[...] * inner[...] * outer[...]
    at = 0
    for v, count, start in ((mix, 2, f * 8), (up[...], 6, f * 24), (out[...], 4, y * 64), (down[...], 4, y * 64)):
        n = v.shape[1]
        line[...] = jnp.zeros((8, 128), F32)
        line[:, 0:n] = jnp.broadcast_to(v, (8, n))
        turned = pltpu.roll(line[...], lax.rem(start, 128), 1)
        for r in range(count):
            place = lane + r * 128
            row = jnp.where((place >= start) & (place < start + n), turned, 0.0)
            rows[at + r : at + r + 1, :] = row[0:1]
        at += count
    left = rows[...]
    for i in range(3):
        part = left.astype(BF)
        left = left - part.astype(F32)
        for k in range(8):
            copies[k, i * 16 : i * 16 + 16, 512:640] = part
    for k in range(8):
        copies[k, 48:64, 512:640] = jnp.zeros((16, 128), BF)
    copies_kernel(pieces, copies)


def read_scales(vi, mix_cols, up_cols, out_cols, down_cols):
    total = None
    for k in range(4):
        parts = vi[k][:, 512:640].astype(F32).reshape(8, 64, 128).sum(axis=0)
        rows = parts[0:16] + parts[16:32] + parts[32:48]
        total = rows if total is None else total + rows
        for i in range(4):
            at = slice(k * 512 + i * 128, k * 512 + i * 128 + 128)
            out_cols[:, at] = rows[8 + i : 9 + i]
            down_cols[:, at] = rows[12 + i : 13 + i]
    for i in range(2):
        mix_cols[:, i * 128 : i * 128 + 128] = total[i : i + 1]
    for i in range(6):
        up_cols[:, i * 128 : i * 128 + 128] = total[2 + i : 3 + i]


def mlp_cast_kernel(pieces, up, down):
    copies_kernel(pieces[:1], up)
    w, copy = pieces[1]
    copy.wait()
    down[...] = w[...].astype(BF)


def side_kernel(pieces, both):
    at = 0
    for w, copy in pieces:
        copy.wait()
        both[:, at : at + w.shape[1]] = w[...].astype(BF)
        at += w.shape[1]


def stack_kernel(first, second, third, fourth, stacked):
    for i, w in enumerate((first, second, third, fourth)):
        stacked[i * 64 : i * 64 + 64, :] = w[...]


def norm_kernel(where, tokens, gain, normed, share):
    z, row = where[0], where[1] * 4 + where[2]
    t = tokens[...].astype(F32)
    scale = lax.rsqrt(jnp.mean(t * t, axis=-1, keepdims=True) + norm_eps)
    for k in range(4):
        at = slice(k * 512, k * 512 + 512)
        normed[:, at] = (tokens[:, block(z, k)].astype(F32) * scale * gain[:, block(z, k)]).astype(BF)
        share[:, at] = tokens[rows_of(row, 48), block(z, k)].astype(F32)


def conv_kernel(normed, taps, vi, conv, cols, up_cols, out_cols, down_cols, padded):
    read_scales(vi, cols, up_cols, out_cols, down_cols)
    value = times_rows(normed, vi, slice(0, 256))
    inner = times_rows(normed, vi, slice(256, 512))
    gated = inner * value
    padded[0:8, :] = jnp.zeros((8, 256), F32)
    padded[392:400, :] = jnp.zeros((8, 256), F32)
    padded[8:392, :] = gated
    mixed = taps[0:1, :] * padded[7:391, :] + taps[1:2, :] * gated + taps[2:3, :] * padded[9:393, :]
    conv[...] = mixed * cols[...]


def z_piece(w, k, at, n):
    return w[:, k, :, at : at + n].reshape(512, n)


def hidden_kernel(where, normed, conv, oo, hidden, other):
    outer = times_rows(normed, [z_piece(oo[0], k, 0, 256) for k in range(4)], slice(0, 256))
    hidden[...] = (outer * conv[...]).astype(BF)
    theirs = hidden[rows_of(1 - where[1], 192), :]
    for k, (at, size) in enumerate(SPANS):
        other[:, at : at + size] = dot_t(theirs, z_piece(oo[0], k, 256, 256)).astype(BF)


def mix_kernel(where, hidden, got, oo, mix):
    mine = hidden[rows_of(where[1], 192), :]
    for k, (at, size) in enumerate(SPANS):
        part = dot_t(mine, z_piece(oo[0], k, 256, 256))
        mix[:, at : at + size] = (part + got[:, at : at + size].astype(F32)).astype(BF)


def middle_kernel(where, share, got, cols, gain, middle, copies):
    z = where[0]
    total = got[0].astype(F32) + got[1].astype(F32) + got[2].astype(F32) + got[3].astype(F32)
    mid = share[...] + total * cols[...]
    middle[...] = mid
    scale = lax.rsqrt(jnp.mean(mid * mid, axis=-1, keepdims=True) + norm_eps)
    for k in range(4):
        at = slice(k * 512, k * 512 + 512)
        part = (mid[:, at] * scale * gain[:, block(z, k)]).astype(BF)
        for j in range(4):
            copies[j, :, at] = part


def act_of(rows, ud, cols, act):
    @pl.loop(0, 3)
    def _(i):
        at = pl.ds(pl.multiple_of(i * 256, 256), 256)
        up = times_rows(rows, ud, at) * cols[:, at]
        act[:, at] = jnp.square(jnp.maximum(up, 0.0)).astype(BF)


def up_kernel(rows, cols, ud, act):
    act_of(rows, ud, cols, act)


def down_parts(act, down):
    for k, (at, size) in enumerate(SPANS):
        yield slice(at, at + size), dot_t(act[...], z_piece(down, k, 0, 768))


def up_down_kernel(cols, late, other, act, total):
    rows, rows_copy = late[0]
    rows_copy.wait()
    for k, ((at, size), (p, copy)) in enumerate(zip(SPANS, late[1:])):
        copy.wait()
        for n in range(0, 768, 256):
            part = dot(rows[:, at : at + size], p[:, n : n + 256])
            if k:
                part = part + total[:, n : n + 256]
            if k < 3:
                total[:, n : n + 256] = part
            else:
                up = part * cols[:, n : n + 256]
                act[:, n : n + 256] = jnp.square(jnp.maximum(up, 0.0)).astype(BF)
    down, copy = late[5]
    copy.wait()
    for at, part in down_parts(act, down):
        other[:, at] = part.astype(BF)


def down_kernel(act, got, pieces, mlp):
    for at, part in down_parts(act, pieces[0]):
        mlp[:, at] = (part + got[:, at].astype(F32)).astype(BF)


def end_kernel(where, middle, got, cols, copies):
    z = where[0]
    total = got[0].astype(F32) + got[1].astype(F32) + got[2].astype(F32) + got[3].astype(F32)
    end = (middle[...] + total * cols[...]).astype(BF)
    for k in range(4):
        for j in range(4):
            copies[j, :, block(z, k)] = end[:, k * 512 : k * 512 + 512]


def join_kernel(where, mine, theirs, result):
    result[rows_of(where[1], 192), :] = mine[...]
    result[rows_of(1 - where[1], 192), :] = theirs[...]


def body(
    tokens,
    mix_gain,
    value_weight,
    value_scale,
    inner_weight,
    inner_scale,
    outer_weight,
    outer_scale,
    conv_taps,
    out_weight,
    out_scale,
    mlp_gain,
    up_weight,
    up_scale,
    down_weight,
    down_scale,
):
    z = lax.axis_index("zl")
    where = jnp.stack([z, lax.axis_index("c"), lax.axis_index("x"), lax.axis_index("y")]).astype(jnp.int32)

    vi = jnp.concatenate([value_weight.astype(BF), inner_weight.astype(BF)], axis=1)
    small = (value_scale, inner_scale, outer_scale, up_scale, out_scale, down_scale)
    vi = kernel(
        copies_scales_kernel,
        SHAPE((8, 64, 640), BF),
        1_000_000,
        where,
        *[v[None] for v in small],
        late=[value_weight, inner_weight],
        scratch=[pltpu.VMEM((8, 128), F32), pltpu.VMEM((16, 128), F32)],
    )
    vi = spread(vi, "y").reshape(512, 640)
    oo = kernel(side_kernel, SHAPE((64, 512), BF), 1_000_000, late=[outer_weight, out_weight.T])
    up, dn = kernel(
        mlp_cast_kernel,
        (SHAPE((8, 64, 768), BF), SHAPE((64, 768), BF)),
        1_000_000,
        late=[up_weight, down_weight.T],
    )
    oo = z_then_y(oo, 2)
    up = spread(up, "y").reshape(512, 768)
    dn = z_then_y(dn, -2)
    normed, share = kernel(
        norm_kernel,
        (SHAPE((384, 2048), BF), SHAPE((48, 2048), F32)),
        10_000_000,
        where,
        tokens[0],
        mix_gain[None],
    )
    vi = along_z(vi, 1)
    up = along_z(up, 1)

    wide = SHAPE((1, 2048), F32)
    conv, _, up_cols, out_cols, down_cols = kernel(
        conv_kernel,
        (SHAPE((384, 256), F32), SHAPE((1, 256), F32), SHAPE((1, 768), F32), wide, wide),
        800_000_000,
        normed,
        conv_taps,
        weights=vi,
        scratch=[pltpu.VMEM((400, 256), F32)],
    )
    hidden, mix_other = kernel(
        hidden_kernel,
        (SHAPE((384, 256), BF), SHAPE((192, 2048), BF)),
        600_000_000,
        where,
        normed,
        conv,
        weights=[oo],
    )
    got = swap_cores(mix_other)
    mix = kernel(mix_kernel, SHAPE((192, 2048), BF), 200_000_000, where, hidden, got, weights=[oo])
    mix = spread(mix.reshape(4, 48, 2048), "x")
    middle, copies = kernel(
        middle_kernel,
        (SHAPE((48, 2048), F32), SHAPE((4, 48, 2048), BF)),
        2_000_000,
        where,
        share,
        mix,
        out_cols,
        mlp_gain[None],
    )
    own = spread(copies, "x").reshape(192, 2048)
    other = swap_cores(own)
    act = kernel(up_kernel, SHAPE((192, 768), BF), 600_000_000, own, up_cols, weights=up)
    mlp_other = kernel(
        up_down_kernel,
        SHAPE((192, 2048), BF),
        1_200_000_000,
        up_cols,
        late=[other, *up, dn],
        scratch=[pltpu.VMEM((192, 768), BF), pltpu.VMEM((192, 768), F32)],
    )
    got = swap_cores(mlp_other)
    mlp = kernel(down_kernel, SHAPE((192, 2048), BF), 600_000_000, act, got, weights=[dn])
    mlp = spread(mlp.reshape(4, 48, 2048), "x")
    copies = kernel(end_kernel, SHAPE((4, 48, 2048), BF), 2_000_000, where, middle, mlp, down_cols)
    mine = spread(copies, "x").reshape(192, 2048)
    theirs = swap_cores(mine)
    result = kernel(join_kernel, SHAPE((384, 2048), BF), 1_000_000, where, mine, theirs)
    return result[None]


def solution(mesh):
    fine = Mesh(mesh.devices.reshape(2, 4, 8, 4, 2), ("zh", "zl", "y", "x", "c"))
    rows = P(("zh", "zl", "y"), None, None)
    fs, tp = ("zl", "y"), ("x", "c")
    all_cols = P(tp + fs)
    placed = (
        rows,
        P(),
        P(fs, tp),
        all_cols,
        P(fs, tp),
        all_cols,
        P(fs, tp),
        all_cols,
        P(None, tp),
        P(tp, fs),
        P(fs),
        P(),
        P(fs, tp),
        all_cols,
        P(tp, fs),
        P(fs),
    )
    return jax.shard_map(body, mesh=fine, in_specs=placed, out_specs=rows, check_vma=False)
```

```python
import jax
import jax.numpy as jnp
from jax import lax
from jax.experimental import pallas as pl
from jax.experimental.pallas import tpu as pltpu
from jax.sharding import Mesh, PartitionSpec as P


norm_eps = 1e-06

Z = ("zh", "zl")
BF = jnp.bfloat16
F32 = jnp.float32
SHAPE = jax.ShapeDtypeStruct


def z_shift(a, step):
    return lax.ppermute(a, Z, [(i, (i + step) % 8) for i in range(8)])


def swap_cores(a):
    return lax.ppermute(a, "c", [(0, 1), (1, 0)])


def spread(a, axis):
    return lax.all_to_all(a, axis, 0, 0, tiled=True)


def along_z(got, far):
    before = z_shift(got, 1)
    after = z_shift(got, -1)
    return [got, after, z_shift(before if far > 0 else after, far), before]


def along_z_halves(got):
    half = got.shape[0] // 2
    before = z_shift(got, 1)
    after = z_shift(got, -1)
    low = z_shift(before[:half], 1)
    return [got, after, low, z_shift(after[half:], -1), before]


def z_then_y(a, far):
    near = [z_shift(a, step) for step in (-1, far, 1)]
    width = a.shape[1]
    stacked = kernel(stack_kernel, SHAPE((256, width), BF), 1_000_000, a, *near)
    return lax.all_gather(stacked, "y", axis=0, tiled=True).reshape(8, 4, 64, width)


def kernel(body, outs, flops, *args, weights=(), late=(), scratch=()):
    spaces = [pltpu.SMEM if a.dtype == jnp.int32 else pltpu.VMEM for a in (*args, *weights)]
    spaces += [pl.ANY] * len(late)
    moved = sum(a.size * a.dtype.itemsize for a in (*args, *weights, *late))
    held = [pltpu.VMEM(w.shape, w.dtype) for w in late]
    held += [pltpu.SemaphoreType.DMA((len(late),))] if late else []
    count, n_out = len(args), len(jax.tree.leaves(outs))

    def run(*refs):
        given, first, end = list(refs[:count]), count + len(weights), count + len(weights) + len(late)
        if weights:
            given.append(list(refs[count:first]))
        inner = refs[end + n_out :]
        if late:
            near, sem, inner = inner[: len(late)], inner[len(late)], inner[len(late) + 1 :]
            pairs = enumerate(zip(refs[first:end], near))
            copies = [pltpu.make_async_copy(f, v, sem.at[i]) for i, (f, v) in pairs]
            for copy in copies:
                copy.start()
            given.append(list(zip(near, copies)))
        body(*given, *refs[end : end + n_out], *inner)

    return pl.pallas_call(
        run,
        out_shape=outs,
        in_specs=[pl.BlockSpec(memory_space=s) for s in spaces],
        out_specs=jax.tree.map(lambda _: pl.BlockSpec(memory_space=pltpu.VMEM), outs),
        scratch_shapes=[*held, *scratch],
        cost_estimate=pl.CostEstimate(flops=flops, bytes_accessed=moved, transcendentals=0),
        compiler_params=pltpu.CompilerParams(
            vmem_limit_bytes=(20 if weights or not late else 60) * 1024 * 1024
        ),
    )(*args, *weights, *late)


def dot(a, b):
    return jnp.dot(a, b, preferred_element_type=F32)


def dot_t(a, b):
    return lax.dot_general(a, b, (((1,), (1,)), ((), ())), preferred_element_type=F32)


SPANS = ((0, 512), (512, 512), (1024, 512), (1536, 512))


def block(z, k):
    return pl.ds(pl.multiple_of(lax.rem(z + k, 4) * 512, 512), 512)


def rows_of(index, count):
    return pl.ds(pl.multiple_of(index * count, 16), count)


def times_rows(a, pieces, cols):
    total, at = None, 0
    for p in pieces:
        part = dot(a[:, at : at + p.shape[0]], p[:, cols])
        total = part if total is None else total + part
        at += p.shape[0]
    return total


def copies_kernel(pieces, copies):
    at = 0
    for w, copy in pieces:
        copy.wait()
        part, width = w[...].astype(BF), w.shape[1]
        for y in range(8):
            copies[y, :, at : at + width] = part
        at += width


def copies_scales_kernel(where, value, inner, outer, up, out, down, pieces, copies, line, rows):
    y = where[3]
    f = where[0] * 8 + y
    lane = lax.broadcasted_iota(jnp.int32, (8, 128), 1)
    mix = value[...] * inner[...] * outer[...]
    at = 0
    for v, count, start in ((mix, 2, f * 8), (up[...], 6, f * 24), (out[...], 4, y * 64), (down[...], 4, y * 64)):
        n = v.shape[1]
        line[...] = jnp.zeros((8, 128), F32)
        line[:, 0:n] = jnp.broadcast_to(v, (8, n))
        turned = pltpu.roll(line[...], lax.rem(start, 128), 1)
        for r in range(count):
            place = lane + r * 128
            row = jnp.where((place >= start) & (place < start + n), turned, 0.0)
            rows[at + r : at + r + 1, :] = row[0:1]
        at += count
    left = rows[...]
    for i in range(3):
        part = left.astype(BF)
        left = left - part.astype(F32)
        for k in range(8):
            copies[k, i * 16 : i * 16 + 16, 512:640] = part
    for k in range(8):
        copies[k, 48:64, 512:640] = jnp.zeros((16, 128), BF)
    copies_kernel(pieces, copies)


def read_scales(vi, mix_cols, up_cols, out_cols, down_cols):
    total = None
    for k in range(4):
        parts = vi[k][:, 512:640].astype(F32).reshape(8, 64, 128).sum(axis=0)
        rows = parts[0:16] + parts[16:32] + parts[32:48]
        total = rows if total is None else total + rows
        for i in range(4):
            at = slice(k * 512 + i * 128, k * 512 + i * 128 + 128)
            out_cols[:, at] = rows[8 + i : 9 + i]
            down_cols[:, at] = rows[12 + i : 13 + i]
    for i in range(2):
        mix_cols[:, i * 128 : i * 128 + 128] = total[i : i + 1]
    for i in range(6):
        up_cols[:, i * 128 : i * 128 + 128] = total[2 + i : 3 + i]


def mlp_cast_kernel(pieces, up, down):
    copies_kernel(pieces[:1], up)
    w, copy = pieces[1]
    copy.wait()
    down[...] = w[...].astype(BF)


def side_kernel(pieces, both):
    at = 0
    for w, copy in pieces:
        copy.wait()
        both[:, at : at + w.shape[1]] = w[...].astype(BF)
        at += w.shape[1]


def stack_kernel(first, second, third, fourth, stacked):
    for i, w in enumerate((first, second, third, fourth)):
        stacked[i * 64 : i * 64 + 64, :] = w[...]


def norm_kernel(where, tokens, gain, normed, share):
    z, row = where[0], where[1] * 4 + where[2]
    t = tokens[...].astype(F32)
    scale = lax.rsqrt(jnp.mean(t * t, axis=-1, keepdims=True) + norm_eps)
    for k in range(4):
        at = slice(k * 512, k * 512 + 512)
        normed[:, at] = (tokens[:, block(z, k)].astype(F32) * scale * gain[:, block(z, k)]).astype(BF)
        share[:, at] = tokens[rows_of(row, 48), block(z, k)].astype(F32)


def conv_kernel(normed, taps, vi, conv, cols, up_cols, out_cols, down_cols, padded):
    read_scales(vi, cols, up_cols, out_cols, down_cols)
    value = times_rows(normed, vi, slice(0, 256))
    inner = times_rows(normed, vi, slice(256, 512))
    gated = inner * value
    padded[0:8, :] = jnp.zeros((8, 256), F32)
    padded[392:400, :] = jnp.zeros((8, 256), F32)
    padded[8:392, :] = gated
    mixed = taps[0:1, :] * padded[7:391, :] + taps[1:2, :] * gated + taps[2:3, :] * padded[9:393, :]
    conv[...] = mixed * cols[...]


def z_piece(w, k, at, n):
    return w[:, k, :, at : at + n].reshape(512, n)


def hidden_kernel(where, normed, conv, oo, hidden, other):
    outer = times_rows(normed, [z_piece(oo[0], k, 0, 256) for k in range(4)], slice(0, 256))
    hidden[...] = (outer * conv[...]).astype(BF)
    theirs = hidden[rows_of(1 - where[1], 192), :]
    for k, (at, size) in enumerate(SPANS):
        other[:, at : at + size] = dot_t(theirs, z_piece(oo[0], k, 256, 256)).astype(BF)


def mix_kernel(where, hidden, got, oo, mix):
    mine = hidden[rows_of(where[1], 192), :]
    for k, (at, size) in enumerate(SPANS):
        part = dot_t(mine, z_piece(oo[0], k, 256, 256))
        mix[:, at : at + size] = (part + got[:, at : at + size].astype(F32)).astype(BF)


def middle_kernel(where, share, got, cols, gain, middle, copies):
    z = where[0]
    total = got[0].astype(F32) + got[1].astype(F32) + got[2].astype(F32) + got[3].astype(F32)
    mid = share[...] + total * cols[...]
    middle[...] = mid
    scale = lax.rsqrt(jnp.mean(mid * mid, axis=-1, keepdims=True) + norm_eps)
    for k in range(4):
        at = slice(k * 512, k * 512 + 512)
        part = (mid[:, at] * scale * gain[:, block(z, k)]).astype(BF)
        for j in range(4):
            copies[j, :, at] = part


def act_of(rows, ud, cols, act):
    @pl.loop(0, 3)
    def _(i):
        at = pl.ds(pl.multiple_of(i * 256, 256), 256)
        up = times_rows(rows, ud, at) * cols[:, at]
        act[:, at] = jnp.square(jnp.maximum(up, 0.0)).astype(BF)


def up_kernel(rows, cols, ud, act):
    act_of(rows, ud, cols, act)


def down_parts(act, down):
    for k, (at, size) in enumerate(SPANS):
        yield slice(at, at + size), dot_t(act[...], z_piece(down, k, 0, 768))


def up_down_kernel(cols, late, other, act, total):
    rows, rows_copy = late[0]
    rows_copy.wait()
    at = 0
    for k, (p, copy) in enumerate(late[1:6]):
        copy.wait()
        size = p.shape[0]
        for n in range(0, 768, 256):
            part = dot(rows[:, at : at + size], p[:, n : n + 256])
            if k:
                part = part + total[:, n : n + 256]
            if k < 4:
                total[:, n : n + 256] = part
            else:
                up = part * cols[:, n : n + 256]
                act[:, n : n + 256] = jnp.square(jnp.maximum(up, 0.0)).astype(BF)
        at += size
    down, copy = late[6]
    copy.wait()
    for at, part in down_parts(act, down):
        other[:, at] = part.astype(BF)


def down_kernel(act, got, pieces, mlp):
    for at, part in down_parts(act, pieces[0]):
        mlp[:, at] = (part + got[:, at].astype(F32)).astype(BF)


def end_kernel(where, middle, got, cols, copies):
    z = where[0]
    total = got[0].astype(F32) + got[1].astype(F32) + got[2].astype(F32) + got[3].astype(F32)
    end = (middle[...] + total * cols[...]).astype(BF)
    for k in range(4):
        for j in range(4):
            copies[j, :, block(z, k)] = end[:, k * 512 : k * 512 + 512]


def join_kernel(where, mine, theirs, result):
    result[rows_of(where[1], 192), :] = mine[...]
    result[rows_of(1 - where[1], 192), :] = theirs[...]


def body(
    tokens,
    mix_gain,
    value_weight,
    value_scale,
    inner_weight,
    inner_scale,
    outer_weight,
    outer_scale,
    conv_taps,
    out_weight,
    out_scale,
    mlp_gain,
    up_weight,
    up_scale,
    down_weight,
    down_scale,
):
    z = lax.axis_index("zl")
    where = jnp.stack([z, lax.axis_index("c"), lax.axis_index("x"), lax.axis_index("y")]).astype(jnp.int32)

    vi = jnp.concatenate([value_weight.astype(BF), inner_weight.astype(BF)], axis=1)
    small = (value_scale, inner_scale, outer_scale, up_scale, out_scale, down_scale)
    vi = kernel(
        copies_scales_kernel,
        SHAPE((8, 64, 640), BF),
        1_000_000,
        where,
        *[v[None] for v in small],
        late=[value_weight, inner_weight],
        scratch=[pltpu.VMEM((8, 128), F32), pltpu.VMEM((16, 128), F32)],
    )
    vi = spread(vi, "y").reshape(512, 640)
    oo = kernel(side_kernel, SHAPE((64, 512), BF), 1_000_000, late=[outer_weight, out_weight.T])
    up, dn = kernel(
        mlp_cast_kernel,
        (SHAPE((8, 64, 768), BF), SHAPE((64, 768), BF)),
        1_000_000,
        late=[up_weight, down_weight.T],
    )
    oo = z_then_y(oo, 2)
    up = spread(up, "y").reshape(512, 768)
    dn = z_then_y(dn, -2)
    normed, share = kernel(
        norm_kernel,
        (SHAPE((384, 2048), BF), SHAPE((48, 2048), F32)),
        10_000_000,
        where,
        tokens[0],
        mix_gain[None],
    )
    vi = along_z(vi, 1)
    up = along_z_halves(up)

    wide = SHAPE((1, 2048), F32)
    conv, _, up_cols, out_cols, down_cols = kernel(
        conv_kernel,
        (SHAPE((384, 256), F32), SHAPE((1, 256), F32), SHAPE((1, 768), F32), wide, wide),
        800_000_000,
        normed,
        conv_taps,
        weights=vi,
        scratch=[pltpu.VMEM((400, 256), F32)],
    )
    hidden, mix_other = kernel(
        hidden_kernel,
        (SHAPE((384, 256), BF), SHAPE((192, 2048), BF)),
        600_000_000,
        where,
        normed,
        conv,
        weights=[oo],
    )
    got = swap_cores(mix_other)
    mix = kernel(mix_kernel, SHAPE((192, 2048), BF), 200_000_000, where, hidden, got, weights=[oo])
    mix = spread(mix.reshape(4, 48, 2048), "x")
    middle, copies = kernel(
        middle_kernel,
        (SHAPE((48, 2048), F32), SHAPE((4, 48, 2048), BF)),
        2_000_000,
        where,
        share,
        mix,
        out_cols,
        mlp_gain[None],
    )
    own = spread(copies, "x").reshape(192, 2048)
    other = swap_cores(own)
    act = kernel(up_kernel, SHAPE((192, 768), BF), 600_000_000, own, up_cols, weights=up)
    mlp_other = kernel(
        up_down_kernel,
        SHAPE((192, 2048), BF),
        1_200_000_000,
        up_cols,
        late=[other, *up, dn],
        scratch=[pltpu.VMEM((192, 768), BF), pltpu.VMEM((192, 768), F32)],
    )
    got = swap_cores(mlp_other)
    mlp = kernel(down_kernel, SHAPE((192, 2048), BF), 600_000_000, act, got, weights=[dn])
    mlp = spread(mlp.reshape(4, 48, 2048), "x")
    copies = kernel(end_kernel, SHAPE((4, 48, 2048), BF), 2_000_000, where, middle, mlp, down_cols)
    mine = spread(copies, "x").reshape(192, 2048)
    theirs = swap_cores(mine)
    result = kernel(join_kernel, SHAPE((384, 2048), BF), 1_000_000, where, mine, theirs)
    return result[None]


def solution(mesh):
    fine = Mesh(mesh.devices.reshape(2, 4, 8, 4, 2), ("zh", "zl", "y", "x", "c"))
    rows = P(("zh", "zl", "y"), None, None)
    fs, tp = ("zl", "y"), ("x", "c")
    all_cols = P(tp + fs)
    placed = (
        rows,
        P(),
        P(fs, tp),
        all_cols,
        P(fs, tp),
        all_cols,
        P(fs, tp),
        all_cols,
        P(None, tp),
        P(tp, fs),
        P(fs),
        P(),
        P(fs, tp),
        all_cols,
        P(tp, fs),
        P(fs),
    )
    return jax.shard_map(body, mesh=fine, in_specs=placed, out_specs=rows, check_vma=False)
```
